256 devices in a mesh: sp: 128 (over z, y, x), tp: 2 (over core).
Axes of the slice: x: 4, y: 4, z: 8, core: 2. Of those that a mesh axis runs over, the one named last changes fastest.
Arguments:
- conv_value: bfloat16 [65536, 1536], P('sp', 'tp'), may hold values from -6 to 6
- conv_gate: bfloat16 [65536, 1536], P('sp', 'tp'), may hold values from -8 to 8
- conv_out: bfloat16 [65536, 1536], P('sp', 'tp'), may hold values from -40 to 40
- conv_taps: bfloat16 [31, 1536], P(None, 'tp'), may hold values from -1 to 1
- norm_gain: float32 [1536], P('tp'), may hold values from 0.1 to 1.9
- norm_shift: float32 [1536], P('tp'), may hold values from -3 to 3
- proj_weight: bfloat16 [2048, 1536], P(None, 'tp'), may hold values from -0.15625 to 0.15625
- out_grad: bfloat16 [65536, 2048], P('sp'), may hold values from -24 to 24
Outputs:
- grad_value: bfloat16 [65536, 1536], P('sp', 'tp')
- grad_gate: bfloat16 [65536, 1536], P('sp', 'tp')
- grad_taps: float32 [31, 1536], P(None, 'tp')
- grad_gain: float32 [1536], P('tp')
- grad_shift: float32 [1536], P('tp')
- grad_proj: float32 [2048, 1536], P('sp', 'tp')
The draws below stay inside these ranges and needn't reach their ends.
All inputs are finite; a program needn't handle non-finite values.
Results may differ from the reference program's by a relative error of at most 0.005.
Values may be sent and summed in bfloat16 or wider, within the bound.
A program may use at most 64 MiB of HBM per device.

```python
import jax
import jax.numpy as jnp
from jax import lax

D = 2048
CH = 1536
TAPS = 31
SEQ = 65536


def draw_conv_out(key, part):
    key_scale, key_group, key_base, key_mean = jax.random.split(key, 4)
    chan_scale = jnp.exp(jax.random.uniform(key_scale, (CH,), jnp.float32, -1.0, 1.0))
    group_scale = jnp.exp(jax.random.uniform(key_group, (8,), jnp.float32, -1.2, 1.2))
    group_index = jnp.arange(CH) * 8 // CH
    scales = chan_scale * group_scale[group_index]
    base = jax.random.normal(key_base, (SEQ, CH), jnp.float32) * scales
    offset = jax.random.normal(key_mean, (SEQ, 1), jnp.float32)
    return jnp.clip(base + offset, -40.0, 40.0).astype(jnp.bfloat16)


def spiked(values, rng, source, target, parts, factor):
    def block_of(position):
        return (jnp.arange(values.shape[position]) // (values.shape[position] // parts)).reshape((-1,) + (1,) * (values.ndim - 1 - position))

    one_side = jax.random.permutation(rng, parts)[block_of(target)]
    other_side = (block_of(target) + parts // 2) % parts
    return jnp.where((block_of(source) == one_side) | (block_of(source) == other_side), factor * values, values)


def steps_of(stream_key, extent, shards, smallest, high):
    def one(axis_at, parts):
        steps = jax.random.uniform(jax.random.fold_in(jax.random.fold_in(stream_key, 6), axis_at), (parts,), jnp.float32, smallest / len(shards), high / len(shards))
        return jnp.repeat(jnp.exp(steps), extent[axis_at] // parts).reshape((-1,) + (1,) * (len(extent) - axis_at - 1))

    factor_of = one(*shards[0])
    for cut in shards[1:]:
        factor_of = factor_of * one(*cut)
    return factor_of


def bell_draw(own_key, dims, scale, limit, cuts=(), held_as=jnp.bfloat16):
    entries = jax.random.normal(own_key, dims, jnp.float32) * scale
    if len(cuts) > 0:
        entries = steps_of(own_key, dims, cuts, -0.22, 0.18) * entries
    return jnp.clip(entries, min=-limit, max=limit).astype(held_as)


def noise_with(key, extent, spread, reach, pieces, heavy, held_as=jnp.bfloat16):
    drawn = spread * jax.random.normal(key, extent, jnp.float32)
    if pieces:
        drawn = drawn * steps_of(key, extent, pieces, -0.22, 0.18)
    return jnp.clip(spiked(drawn, jax.random.fold_in(key, 3), *heavy), -reach, reach).astype(held_as)


def setup_inputs(seed: int = 0) -> dict:
    splits = jax.random.split(jax.random.key(seed), 9)
    return {
        "conv_value": bell_draw(splits[0], (SEQ, CH), 1.0, 6.0, ((0, 128), (1, 2))),
        "conv_gate": bell_draw(splits[1], (SEQ, CH), 1.5, 8.0, ((0, 128), (1, 2))),
        "conv_out": draw_conv_out(jax.random.fold_in(splits[8], 71), 0),
        "conv_taps": bell_draw(splits[3], (TAPS, CH), TAPS ** -0.5, 1.0, ((1, 2),)),
        "norm_gain": jnp.clip(1.0 + 0.18 * jax.random.normal(splits[4], (CH,), jnp.float32), 0.1, 1.9),
        "norm_shift": bell_draw(splits[5], (CH,), 0.5, 3.0, ((0, 2),), jnp.float32),
        "proj_weight": bell_draw(splits[6], (D, CH), CH ** -0.5, 0.15625, ((1, 2),)),
        "out_grad": noise_with(splits[7], (SEQ, D), 1.0, 24.0, ((0, 128),), (0, 1, 128, 5.5)),
    }


norm_eps = 1e-05

def reference(conv_value, conv_gate, conv_out, conv_taps, norm_gain, norm_shift, proj_weight, out_grad):
    height = conv_out.astype(jnp.float32)
    center = lax.optimization_barrier(jnp.mean(height, axis=1, keepdims=True))
    centered = height - center
    variance = lax.optimization_barrier(jnp.mean(centered * centered, axis=1, keepdims=True))
    inv_std = lax.rsqrt(variance + norm_eps)
    normed = centered * inv_std
    shifted = normed * norm_gain + norm_shift
    sig_norm = jax.nn.sigmoid(shifted)
    active = (shifted * sig_norm).astype(jnp.bfloat16)
    grad_proj = jnp.dot(out_grad.T, active, preferred_element_type=jnp.float32)
    act_grad = jnp.dot(out_grad, proj_weight, preferred_element_type=jnp.float32)
    norm_grad = act_grad * (sig_norm * (1.0 + shifted * (1.0 - sig_norm)))
    grad_gain = lax.optimization_barrier(jnp.sum(norm_grad * normed, axis=0))
    grad_shift = lax.optimization_barrier(jnp.sum(norm_grad, axis=0))
    scaled = norm_grad * norm_gain
    height_grad = inv_std * (scaled - lax.optimization_barrier(jnp.mean(scaled, axis=1, keepdims=True)) - normed * lax.optimization_barrier(jnp.mean(scaled * normed, axis=1, keepdims=True)))
    sig_gate = jax.nn.sigmoid(conv_gate.astype(jnp.float32))
    value_float = conv_value.astype(jnp.float32)
    gated_rows = lax.optimization_barrier((value_float * sig_gate).astype(jnp.bfloat16)).astype(jnp.float32)
    tap_reach = TAPS - 1
    padded_rows = jnp.pad(gated_rows, ((tap_reach, 0), (0, 0)))
    padded_grad = jnp.pad(height_grad, ((0, tap_reach), (0, 0)))
    tap_values = conv_taps.astype(jnp.float32)
    tap_list = []
    gated_grad = jnp.zeros_like(height_grad)
    for tap_index in range(TAPS):
        tap_list.append(lax.optimization_barrier(jnp.sum(height_grad * padded_rows[tap_index:tap_index + SEQ], axis=0)))
        begin = tap_reach - tap_index
        gated_grad = gated_grad + tap_values[tap_index] * padded_grad[begin:begin + SEQ]
    grad_taps = jnp.stack(tap_list)
    grad_value = (gated_grad * sig_gate).astype(jnp.bfloat16)
    grad_gate = (gated_grad * value_float * sig_gate * (1.0 - sig_gate)).astype(jnp.bfloat16)
    return (grad_value, grad_gate, grad_taps, grad_gain, grad_shift, grad_proj)
```

```python
import jax
import jax.numpy as jnp
from jax import lax
from jax.experimental import pallas as pl
from jax.experimental.pallas import tpu as pltpu
from jax.sharding import Mesh
from jax.sharding import PartitionSpec as P

SP = ("sp_0", "sp_1", "sp_2")
MESH = pl.DeviceIdType.MESH
F32, BF16 = jnp.float32, jnp.bfloat16

norm_eps = 1e-05
LANES = 128
HALO = 32
AUX = 40
NX = NY = 4
NZ = 8
PLANE = NX * NY


def sigmoid(v):
    return 0.5 + 0.5 * jnp.tanh(0.5 * v)


def kernel(
    value_h, gate_h, out_h, taps_h, gain_h, shift_h, weight_h, og_h,
    gv_h, gg_h, gtaps_o, ggain_o, gshift_o, gproj_o,
    value_v, gate_v, out_v, taps_v, gain_v, shift_v, weight_v, og_v, in_sem,
    st_a, st_b, cen_b, inv_b, act_v, fac_v, sc_v, hg, gt, tapsf,
    gx, r1x, r2x, r3x, mx, hx, s1x, s2x, s3x, mx2, ex, zx,
    gy, r1y, r2y, r3y, my, hy, s1y, s2y, s3y, my2, ey, zy,
    red, red_r, zred, ag,
    st_sem, halo_sem, rs_send, rs_recv, z_send, z_recv, ar_send, ar_recv, gv_v, gg_v, out_sem,
):
    rows, chans = value_v.shape
    groups = chans // LANES
    taps_n = taps_v.shape[0]
    reach = taps_n - 1
    chan_total = 2.0 * chans
    z, y, x = (lax.axis_index(a) for a in SP)
    core = lax.axis_index("tp")
    place = (z * NY + y) * NX + x
    last = NZ * PLANE

    def at_place(s):
        return {"sp_0": s // PLANE, "sp_1": lax.rem(s // NX, NY), "sp_2": lax.rem(s, NX)}

    nxt = at_place(lax.rem(place + 1, last))
    prv = at_place(lax.rem(place + last - 1, last))

    def load(i, src, dst):
        c = pltpu.make_async_copy(src, dst, in_sem.at[i])
        c.start()
        return c

    def send(src, dst, ss, rs, dev):
        c = pltpu.make_async_remote_copy(
            src_ref=src, dst_ref=dst, send_sem=ss, recv_sem=rs, device_id=dev, device_id_type=MESH
        )
        c.start()
        return c

    c_out = load(0, out_h, out_v)
    c_gain = load(1, gain_h, gain_v)
    c_shift = load(2, shift_h, shift_v)
    c_taps = load(3, taps_h, taps_v)

    barrier = pltpu.get_barrier_semaphore()
    partners = [{"tp": 1 - core}, nxt, prv]
    p_me = y * NX + x
    plane_dev = []
    plane_pos = []
    for k in range(1, PLANE):
        p = lax.rem(p_me + k, PLANE)
        plane_pos.append(p)
        plane_dev.append({"sp_1": p // NX, "sp_2": lax.rem(p, NX)})
    z_pos = [lax.rem(z + k, NZ) for k in range(1, NZ)]
    z_dev = [{"sp_0": p} for p in z_pos]
    partners += plane_dev + z_dev
    for dev in partners:
        pl.semaphore_signal(barrier, inc=1, device_id=dev, device_id_type=MESH)

    c_out.wait()
    c_gate = load(4, gate_h, gate_v)
    c_value = load(5, value_h, value_v)
    c_og = load(6, og_h, og_v)
    c_weight = load(7, weight_h, weight_v)

    def cols(g):
        return slice(g * LANES, (g + 1) * LANES)

    SB = 64

    @pl.loop(0, rows // SB)
    def _(i):
        rs = pl.ds(i * SB, SB)
        v = out_v[rs, :].astype(F32)
        s = jnp.sum(v, axis=1, keepdims=True)
        d = v - s * (1.0 / chans)
        m2 = jnp.sum(d * d, axis=1, keepdims=True)
        lane = lax.broadcasted_iota(jnp.int32, (SB, LANES), 1)
        st_a[0, rs, :] = jnp.where(lane < LANES // 2, s, m2)

    pl.semaphore_wait(barrier, len(partners))
    c_st1 = send(st_a.at[0], st_b.at[0], st_sem.at[0], st_sem.at[1], {"tp": 1 - core})

    c_gate.wait()
    c_value.wait()

    @pl.loop(0, rows // SB)
    def _(i):
        rs = pl.ds(i * SB, SB)
        for g in range(groups):
            gated = value_v[rs, cols(g)].astype(F32) * sigmoid(gate_v[rs, cols(g)].astype(F32))
            gt[g, pl.ds(HALO + i * SB, SB), :] = gated.astype(BF16).astype(F32)

    c_gain.wait()
    c_shift.wait()
    c_taps.wait()
    for g in range(groups):
        tapsf[g, 0:taps_n, :] = taps_v[:, cols(g)].astype(F32)
    c_halo = send(
        gt.at[:, pl.ds(rows, HALO), :], gt.at[:, pl.ds(0, HALO), :],
        halo_sem.at[0], halo_sem.at[1], nxt,
    )
    c_st1.wait()

    @pl.loop(0, rows // SB)
    def _(i):
        rs = pl.ds(i * SB, SB)
        own, peer = st_a[0, rs, :], st_b[0, rs, :]
        s0, m0 = own[:, 0:1], own[:, LANES // 2 : LANES // 2 + 1]
        s1, m1 = peer[:, 0:1], peer[:, LANES // 2 : LANES // 2 + 1]
        ds = s0 - s1
        var = (m0 + m1 + ds * ds * (1.0 / chan_total)) * (1.0 / chan_total)
        inv = lax.rsqrt(var + norm_eps)
        cen = (s0 + s1) * (1.0 / chan_total)
        cen_b[rs, :] = jnp.broadcast_to(cen, (SB, LANES))
        inv_b[rs, :] = jnp.broadcast_to(inv, (SB, LANES))
        for g in range(groups):
            gain = gain_v[:, cols(g)]
            shift = shift_v[:, cols(g)]
            sh = (out_v[rs, cols(g)].astype(F32) - cen) * inv * gain + shift
            sg = sigmoid(sh)
            act_v[rs, cols(g)] = (sh * sg).astype(BF16)
            fac_v[rs, cols(g)] = sg * (1.0 + sh * (1.0 - sg))

    c_og.wait()
    zb = PLANE * 16
    half_c = chans // 2

    @pl.loop(0, NZ)
    def _(zz):
        lhs = og_v[:, pl.ds(pl.multiple_of(zz * zb, zb), zb)]
        part = lax.dot_general(
            lhs, act_v[...], (((0,), (0,)), ((), ())), preferred_element_type=F32
        ).astype(BF16)
        hf, zq = zz // (NZ // 2), lax.rem(zz, NZ // 2)
        for yy in range(NY):
            for xx in range(NX):
                r0 = (yy * NX + xx) * 16
                gx[xx, hf, yy * 4 + zq] = part[r0 : r0 + 16, 0:half_c]
                gy[yy, hf, xx * 4 + zq] = part[r0 : r0 + 16, half_c:]

    DIRS = (1, -1)

    def ring_start(g, r1, r3, axis, pos, base):
        out = []
        for h, d in enumerate(DIRS):
            out.append(send(
                g.at[lax.rem(pos + 2, 4), h], r1.at[h],
                rs_send.at[base + h], rs_recv.at[base + h], {axis: lax.rem(pos + 4 + d, 4)},
            ))
        for h, d in enumerate(DIRS):
            out.append(send(
                g.at[lax.rem(pos + 4 - d, 4), h], r3.at[h],
                rs_send.at[base + 2 + h], rs_recv.at[base + 2 + h], {axis: lax.rem(pos + 4 - d, 4)},
            ))
        return out

    def ring_mid(g, r1, m, r2, first, axis, pos, base):
        out = []
        for h, d in enumerate(DIRS):
            first[h].wait_recv()
            idx = lax.rem(pos + 4 + d, 4)

            @pl.loop(0, r1.shape[1])
            def _(j, h=h, idx=idx):
                m[h, j] = (r1[h, j].astype(F32) + g[idx, h, j].astype(F32)).astype(BF16)

            out.append(send(
                m.at[h], r2.at[h],
                rs_send.at[base + 4 + h], rs_recv.at[base + 4 + h], {axis: idx},
            ))
        return out

    def ring_end(g, r2, r3, first, second, pos, write):
        for h in range(2):
            second[h].wait_recv()
            first[2 + h].wait_recv()

            @pl.loop(0, r2.shape[1])
            def _(j, h=h):
                t = r2[h, j].astype(F32) + r3[h, j].astype(F32) + g[pos, h, j].astype(F32)
                write(h, j, t.astype(BF16))

    fx = ring_start(gx, r1x, r3x, "sp_2", x, 0)
    fy = ring_start(gy, r1y, r3y, "sp_1", y, 6)

    c_weight.wait()
    NB = 256

    @pl.loop(0, chans // NB)
    def _(n):
        cs = pl.ds(pl.multiple_of(n * NB, NB), NB)
        sc_v[:, cs] = jnp.dot(og_v[...], weight_v[:, cs], preferred_element_type=F32)

    zero = jnp.zeros((8, LANES), F32)

    def norm_pass(i, carry):
        rs = pl.ds(i * SB, SB)
        cen, inv = cen_b[rs, :], inv_b[rs, :]
        r_sum = jnp.zeros((SB, LANES), F32)
        r_dot = jnp.zeros((SB, LANES), F32)
        new = []
        for g in range(groups):
            n = sc_v[rs, cols(g)] * fac_v[rs, cols(g)]
            xc = (out_v[rs, cols(g)].astype(F32) - cen) * inv
            nx = n * xc
            new.append(carry[2 * g] + jnp.sum(nx.reshape(SB // 8, 8, LANES), axis=0))
            new.append(carry[2 * g + 1] + jnp.sum(n.reshape(SB // 8, 8, LANES), axis=0))
            sc = n * gain_v[:, cols(g)]
            r_sum = r_sum + sc
            r_dot = r_dot + sc * xc
            sc_v[rs, cols(g)] = sc
        lane = lax.broadcasted_iota(jnp.int32, (SB, LANES), 1)
        st_a[1, rs, :] = jnp.where(
            lane < LANES // 2,
            jnp.sum(r_sum, axis=1, keepdims=True),
            jnp.sum(r_dot, axis=1, keepdims=True),
        )
        return tuple(new)

    sums = lax.fori_loop(0, rows // SB, norm_pass, (zero,) * (2 * groups))
    c_st2 = send(st_a.at[1], st_b.at[1], st_sem.at[2], st_sem.at[3], {"tp": 1 - core})

    def put_row(g, j, row):
        red[(g * AUX + j) // 8, j % 8 : j % 8 + 1, :] = row

    for g in range(groups):
        put_row(g, taps_n, jnp.sum(sums[2 * g], axis=0, keepdims=True))
        put_row(g, taps_n + 1, jnp.sum(sums[2 * g + 1], axis=0, keepdims=True))
        for j in range(taps_n + 2, AUX):
            put_row(g, j, jnp.zeros((1, LANES), F32))
    for t in range(groups * AUX // 8, red.shape[0]):
        red[t] = zero
    c_st2.wait()

    @pl.loop(0, rows // SB)
    def _(i):
        rs = pl.ds(i * SB, SB)
        both = st_a[1, rs, :] + st_b[1, rs, :]
        gs = both[:, 0:1] * (1.0 / chan_total)
        gd = both[:, LANES // 2 : LANES // 2 + 1] * (1.0 / chan_total)
        cen, inv = cen_b[rs, :], inv_b[rs, :]
        for g in range(groups):
            xc = (out_v[rs, cols(g)].astype(F32) - cen) * inv
            hg[g, rs, :] = inv * (sc_v[rs, cols(g)] - gs - xc * gd)

    c_back = send(
        hg.at[:, pl.ds(0, HALO), :], hg.at[:, pl.ds(rows, HALO), :],
        halo_sem.at[2], halo_sem.at[3], prv,
    )

    mid_x = ring_mid(gx, r1x, mx, r2x, fx, "sp_2", x, 0)
    mid_y = ring_mid(gy, r1y, my, r2y, fy, "sp_1", y, 6)

    c_halo.wait_recv()

    @pl.when(place == 0)
    def _():
        gt[:, 0:HALO, :] = jnp.zeros((groups, HALO, LANES), F32)

    @pl.loop(0, groups)
    def _(g):
        def step(t, acc):
            h = hg[g, pl.ds(pl.multiple_of(t * 8, 8), 8), :]
            return tuple(
                acc[j] + h * gt[g, pl.ds(t * 8 + (HALO - reach + j), 8), :] for j in range(taps_n)
            )

        acc = lax.fori_loop(0, rows // 8, step, (zero,) * taps_n)
        for j in range(taps_n):
            red[g * (AUX // 8) + j // 8, j % 8 : j % 8 + 1, :] = jnp.sum(
                acc[j], axis=0, keepdims=True
            )

    ar_a = []
    for k in range(1, PLANE):
        ar_a.append(send(
            red.at[pl.ds(2 * plane_pos[k - 1], 2)], red_r.at[k - 1],
            ar_send.at[k - 1], ar_recv.at[k - 1], plane_dev[k - 1],
        ))

    c_back.wait_recv()

    @pl.when(place == last - 1)
    def _():
        hg[:, rows : rows + HALO, :] = jnp.zeros((groups, HALO, LANES), F32)

    TB = 16

    def gated_part(g):
        weights = [jnp.broadcast_to(tapsf[g, j : j + 1, :], (8, LANES)) for j in range(taps_n)]

        @pl.loop(0, rows // TB)
        def _(t):
            parts = []
            for b in range(TB // 8):
                acc = [None, None]
                for j in range(taps_n):
                    term = weights[j] * hg[g, pl.ds(t * TB + (b * 8 + reach - j), 8), :]
                    acc[j % 2] = term if acc[j % 2] is None else acc[j % 2] + term
                parts.append(acc[0] + acc[1])
            gg = jnp.concatenate(parts, axis=0)
            rs = pl.ds(pl.multiple_of(t * TB, TB), TB)
            sg = sigmoid(gate_v[rs, cols(g)].astype(F32))
            val = value_v[rs, cols(g)].astype(F32)
            gs = gg * sg
            gv_v[rs, cols(g)] = gs.astype(BF16)
            gg_v[rs, cols(g)] = (gs * val * (1.0 - sg)).astype(BF16)

        a = pltpu.make_async_copy(gv_v.at[:, cols(g)], gv_h.at[:, cols(g)], out_sem.at[2 * g])
        b = pltpu.make_async_copy(gg_v.at[:, cols(g)], gg_h.at[:, cols(g)], out_sem.at[2 * g + 1])
        a.start()
        b.start()
        return [a, b]

    outs = []
    for g in range(groups // 2):
        outs += gated_part(g)

    def to_x(h, j, v):
        hx[j // (NZ // 2), h, lax.rem(j, NZ // 2)] = v

    def to_y(h, j, v):
        hy[j // (NZ // 2), h, lax.rem(j, NZ // 2)] = v

    ring_end(gx, r2x, r3x, fx, mid_x, x, to_x)
    f2x = ring_start(hx, s1x, s3x, "sp_1", y, 12)
    ring_end(gy, r2y, r3y, fy, mid_y, y, to_y)
    f2y = ring_start(hy, s1y, s3y, "sp_2", x, 18)

    for g in range(groups // 2, groups):
        outs += gated_part(g)

    for c in ar_a:
        c.wait_recv()

    mine = red[pl.ds(2 * p_me, 2)]
    for k in range(PLANE - 1):
        mine = mine + red_r[k]
    zred[z] = mine
    ar_b = []
    for k in range(1, NZ):
        ar_b.append(send(
            zred.at[z], zred.at[z], ar_send.at[PLANE + k], ar_recv.at[PLANE + k], z_dev[k - 1],
        ))

    m2x = ring_mid(hx, s1x, mx2, s2x, f2x, "sp_1", y, 12)
    m2y = ring_mid(hy, s1y, my2, s2y, f2y, "sp_2", x, 18)

    for c in ar_b:
        c.wait_recv()
    total = zred[0]
    for k in range(1, NZ):
        total = total + zred[k]
    ag[pl.ds(2 * p_me, 2)] = total
    ar_c = []
    for k in range(1, PLANE):
        ar_c.append(send(
            ag.at[pl.ds(2 * p_me, 2)], ag.at[pl.ds(2 * p_me, 2)],
            ar_send.at[PLANE + NZ + k], ar_recv.at[PLANE + NZ + k], plane_dev[k - 1],
        ))

    def e_x(h, j, v):
        ex[h * (NZ // 2) + j] = v

    def e_y(h, j, v):
        ey[h * (NZ // 2) + j] = v

    ring_end(hx, s2x, s3x, f2x, m2x, y, e_x)
    ring_end(hy, s2y, s3y, f2y, m2y, x, e_y)
    zs = []
    for c, (e, zr) in enumerate(((ex, zx), (ey, zy))):
        for k in range(1, NZ):
            zs.append(send(
                e.at[z_pos[k - 1]], zr.at[k - 1],
                z_send.at[c * NZ + k], z_recv.at[c * NZ + k], z_dev[k - 1],
            ))

    for c in ar_c:
        c.wait_recv()
    for g in range(groups):
        for u in range(AUX // 8):
            tile = ag[g * (AUX // 8) + u]
            if u < taps_n // 8:
                gtaps_o[u * 8 : u * 8 + 8, cols(g)] = tile
            elif u == taps_n // 8:
                gtaps_o[u * 8 : taps_n, cols(g)] = tile[0 : taps_n - u * 8]
        for j, o in ((taps_n, ggain_o), (taps_n + 1, gshift_o)):
            o[:, cols(g)] = ag[(g * AUX + j) // 8, j % 8 : j % 8 + 1, :]

    for c in zs:
        c.wait_recv()
    for c, (e, zr) in enumerate(((ex, zx), (ey, zy))):
        t = e[z].astype(F32)
        for k in range(NZ - 1):
            t = t + zr[k].astype(F32)
        gproj_o[:, c * half_c : (c + 1) * half_c] = t

    for c in [c_halo, c_back, *fx, *fy, *mid_x, *mid_y, *f2x, *f2y, *m2x, *m2y, *ar_a, *ar_b, *ar_c, *zs]:
        c.wait_send()
    for c in outs:
        c.wait()


def local(conv_value, conv_gate, conv_out, conv_taps, norm_gain, norm_shift, proj_weight, out_grad):
    rows, chans = conv_value.shape
    taps_n = conv_taps.shape[0]
    d_model = proj_weight.shape[0]
    groups = chans // LANES
    half = chans // 2
    any_s = pl.BlockSpec(memory_space=pl.ANY)
    vm_s = pl.BlockSpec(memory_space=pltpu.VMEM)
    V = pltpu.VMEM
    DMA = pltpu.SemaphoreType.DMA

    def color():
        unit, small = (2, 16, 16, half), (2, 4, 16, half)
        return [
            V((4, 2, 16, 16, half), BF16),
            V(unit, BF16), V(unit, BF16), V(unit, BF16), V(unit, BF16),
            V((4, 2, 4, 16, half), BF16),
            V(small, BF16), V(small, BF16), V(small, BF16), V(small, BF16),
            V((8, 16, half), BF16),
            V((7, 16, half), BF16),
        ]

    scratch = [
        V((rows, chans), BF16), V((rows, chans), BF16), V((rows, chans), BF16),
        V((taps_n, chans), BF16), V((1, chans), F32), V((1, chans), F32),
        V((d_model, chans), BF16), V((rows, d_model), BF16), DMA((8,)),
        V((2, rows, LANES), F32), V((2, rows, LANES), F32), V((rows, LANES), F32), V((rows, LANES), F32),
        V((rows, chans), BF16), V((rows, chans), F32), V((rows, chans), F32),
        V((groups, rows + HALO, LANES), F32), V((groups, rows + HALO, LANES), F32),
        V((groups, 32, LANES), F32),
        *color(), *color(),
        V((32, 8, LANES), F32), V((PLANE - 1, 2, 8, LANES), F32), V((NZ, 2, 8, LANES), F32),
        V((32, 8, LANES), F32),
        DMA((4,)), DMA((4,)), DMA((24,)), DMA((24,)), DMA((2 * NZ,)), DMA((2 * NZ,)),
        DMA((2 * PLANE + NZ,)), DMA((2 * PLANE + NZ,)),
        V((rows, chans), BF16), V((rows, chans), BF16), DMA((2 * groups,)),
    ]
    S = jax.ShapeDtypeStruct
    gv, gg, gtaps, ggain, gshift, gproj = pl.pallas_call(
        kernel,
        name="conv_backward",
        out_shape=(
            S((rows, chans), BF16), S((rows, chans), BF16), S((taps_n, chans), F32),
            S((1, chans), F32), S((1, chans), F32), S((16, chans), F32),
        ),
        in_specs=[any_s] * 8,
        out_specs=(any_s, any_s, vm_s, vm_s, vm_s, vm_s),
        scratch_shapes=scratch,
        compiler_params=pltpu.CompilerParams(
            collective_id=0, has_side_effects=True, vmem_limit_bytes=56 * 1024 * 1024
        ),
    )(
        conv_value, conv_gate, conv_out, conv_taps,
        norm_gain.reshape(1, chans), norm_shift.reshape(1, chans), proj_weight, out_grad,
    )
    return gv, gg, gtaps, ggain.reshape(chans), gshift.reshape(chans), gproj


def solution(mesh):
    split = Mesh(mesh.devices.reshape(8, 4, 4, mesh.shape["tp"]), (*SP, "tp"))
    placed = (
        P(SP, "tp"), P(SP, "tp"), P(SP, "tp"), P(None, "tp"),
        P("tp"), P("tp"), P(None, "tp"), P(SP, None),
    )
    return jax.shard_map(
        local,
        mesh=split,
        in_specs=placed,
        out_specs=(P(SP, "tp"), P(SP, "tp"), P(None, "tp"), P("tp"), P("tp"), P(SP, "tp")),
        check_vma=False,
    )
```

```python
import jax
import jax.numpy as jnp
from jax import lax
from jax.experimental import pallas as pl
from jax.experimental.pallas import tpu as pltpu
from jax.sharding import Mesh
from jax.sharding import PartitionSpec as P

SP = ("sp_0", "sp_1", "sp_2")
MESH = pl.DeviceIdType.MESH
F32, BF16 = jnp.float32, jnp.bfloat16

norm_eps = 1e-05
LANES = 128
HALO = 32
AUX = 40
NX = NY = 4
NZ = 8
PLANE = NX * NY
VMEM_LIMIT = 32 * 1024 * 1024


def sigmoid(v):
    return 0.5 + 0.5 * jnp.tanh(0.5 * v)


def kernel(
    value_h, gate_h, out_h, taps_h, gain_h, shift_h, weight_h, og_h,
    gv_v, gg_v, gtaps_o, ggain_o, gshift_o, gproj_o,
    value_v, gate_v, out_v, taps_v, gain_v, shift_v, weight_v, og_v, in_sem,
    st_a, st_b, cen_b, inv_b, sum_b, dot_b, act_v, fac_v, sc_v, hg, gt, tapsf,
    gx, r1x, r2x, r3x, mx, hx, s1x, s2x, s3x, m2x, ex, zx,
    gy, r1y, r2y, r3y, my, hy, s1y, s2y, s3y, m2y, ey, zy,
    gz, rlz, rsz, mlz, msz, hz, s1z, s2z, s3z, m2z, ez, xz,
    red, red_r, zred, ag,
    st_sem, halo_sem, rs_send, rs_recv, z_send, z_recv, ar_send, ar_recv,
):
    rows, chans = value_v.shape
    groups = chans // LANES
    taps_n = taps_v.shape[0]
    reach = taps_n - 1
    chan_total = 2.0 * chans
    z, y, x = (lax.axis_index(a) for a in SP)
    core = lax.axis_index("tp")
    place = (z * NY + y) * NX + x
    last = NZ * PLANE
    blocks = rows // LANES

    def at_place(s):
        return {"sp_0": s // PLANE, "sp_1": lax.rem(s // NX, NY), "sp_2": lax.rem(s, NX)}

    nxt = at_place(lax.rem(place + 1, last))
    prv = at_place(lax.rem(place + last - 1, last))
    other = {"tp": 1 - core}

    def load(i, src, dst):
        c = pltpu.make_async_copy(src, dst, in_sem.at[i])
        c.start()
        return c

    sent = []

    def send(src, dst, ss, rs, dev):
        c = pltpu.make_async_remote_copy(
            src_ref=src, dst_ref=dst, send_sem=ss, recv_sem=rs, device_id=dev, device_id_type=MESH
        )
        c.start()
        sent.append(c)
        return c

    c_out = load(0, out_h, out_v)
    c_gain = load(1, gain_h, gain_v)
    c_shift = load(2, shift_h, shift_v)
    c_taps = load(3, taps_h, taps_v)
    c_gate = load(4, gate_h, gate_v)
    c_value = load(5, value_h, value_v)

    barrier = pltpu.get_barrier_semaphore()
    p_me = y * NX + x
    plane_dev = []
    plane_pos = []
    for k in range(1, PLANE):
        p = lax.rem(p_me + k, PLANE)
        plane_pos.append(p)
        plane_dev.append({"sp_1": p // NX, "sp_2": lax.rem(p, NX)})
    z_pos = [lax.rem(z + k, NZ) for k in range(1, NZ)]
    z_dev = [{"sp_0": p} for p in z_pos]
    x_pos = [lax.rem(x + k, NX) for k in range(1, NX)]
    x_dev = [{"sp_2": p} for p in x_pos]
    partners = [other, nxt, prv] + plane_dev + z_dev
    for dev in partners:
        pl.semaphore_signal(barrier, inc=1, device_id=dev, device_id_type=MESH)

    c_out.wait()
    c_og = load(6, og_h, og_v)

    def cols(g):
        return slice(g * LANES, (g + 1) * LANES)

    def blk(i):
        return slice(i * LANES, (i + 1) * LANES)

    eye = lax.broadcasted_iota(jnp.int32, (LANES, LANES), 0) == lax.broadcasted_iota(
        jnp.int32, (LANES, LANES), 1
    )
    for i in range(blocks):
        part = out_v[blk(i), cols(0)].astype(F32)
        for g in range(1, groups):
            part = part + out_v[blk(i), cols(g)].astype(F32)
        s = jnp.sum(part, axis=1, keepdims=True)
        m = s * (1.0 / chans)
        d = out_v[blk(i), cols(0)].astype(F32) - m
        sq = d * d
        for g in range(1, groups):
            d = out_v[blk(i), cols(g)].astype(F32) - m
            sq = sq + d * d
        st_a[0, i : i + 1, :] = jnp.sum(jnp.where(eye, s, 0.0), axis=0, keepdims=True)
        st_a[0, blocks + i : blocks + i + 1, :] = jnp.sum(sq.T, axis=0, keepdims=True)

    pl.semaphore_wait(barrier, len(partners))
    c_st1 = send(st_a.at[0], st_b.at[0], st_sem.at[0], st_sem.at[1], other)

    SB = 64
    c_gate.wait()
    c_value.wait()
    c_weight = load(7, weight_h, weight_v)

    @pl.loop(0, rows // SB)
    def _(i):
        rs = pl.ds(i * SB, SB)
        for g in range(groups):
            gated = value_v[rs, cols(g)].astype(F32) * sigmoid(gate_v[rs, cols(g)].astype(F32))
            gt[g, pl.ds(HALO + i * SB, SB), :] = gated.astype(BF16).astype(F32)

    c_gain.wait()
    c_shift.wait()
    c_taps.wait()
    for g in range(groups):
        tapsf[g, 0:taps_n, :] = taps_v[:, cols(g)].astype(F32)
    c_halo = send(
        gt.at[:, pl.ds(rows, HALO), :], gt.at[:, pl.ds(0, HALO), :],
        halo_sem.at[0], halo_sem.at[1], nxt,
    )
    c_st1.wait_recv()

    def spread(dst, src):
        for i in range(blocks):
            dst[blk(i), :] = jnp.broadcast_to(src[i : i + 1, :], (LANES, LANES)).T

    own, peer = st_a[0], st_b[0]
    s0, m0 = own[0:blocks], own[blocks : 2 * blocks]
    s1, m1 = peer[0:blocks], peer[blocks : 2 * blocks]
    ds = s0 - s1
    var = (m0 + m1 + ds * ds * (1.0 / chan_total)) * (1.0 / chan_total)
    spread(cen_b, (s0 + s1) * (1.0 / chan_total))
    spread(inv_b, lax.rsqrt(var + norm_eps))

    @pl.loop(0, rows // SB)
    def _(i):
        rs = pl.ds(i * SB, SB)
        cen, inv = cen_b[rs, :], inv_b[rs, :]
        for g in range(groups):
            sh = (out_v[rs, cols(g)].astype(F32) - cen) * inv * gain_v[g : g + 1, :] + shift_v[g : g + 1, :]
            sg = sigmoid(sh)
            act_v[rs, cols(g)] = (sh * sg).astype(BF16)
            fac_v[rs, cols(g)] = sg * (1.0 + sh * (1.0 - sg))

    c_og.wait()
    zb = PLANE * 16
    third = chans // 3
    HZ = NZ // 2

    def partial(zz, hf, zq):
        lhs = og_v[:, pl.ds(pl.multiple_of(zz * zb, zb), zb)]
        part = lax.dot_general(
            lhs, act_v[...], (((0,), (0,)), ((), ())), preferred_element_type=F32
        ).astype(BF16)
        for yy in range(NY):
            for xx in range(NX):
                r0 = (yy * NX + xx) * 16
                gx[xx, hf, yy * 4 + zq] = part[r0 : r0 + 16, 0:third]
                gy[yy, hf, xx * 4 + zq] = part[r0 : r0 + 16, third : 2 * third]
                gz[zz, yy // 2, (yy % 2) * 4 + xx] = part[r0 : r0 + 16, 2 * third :]

    DIRS = (1, -1)

    def tiles_add(n, step, fn):
        @pl.loop(0, n // step)
        def _(j):
            fn(j, pl.ds(j * step, step))

    class Ring4:
        def __init__(self, g, r1, r2, r3, m, axis, pos, base):
            self.g, self.r1, self.r2, self.r3, self.m = g, r1, r2, r3, m
            self.axis, self.pos, self.base = axis, pos, base
            self.a, self.b, self.c = {}, {}, {}
            self.n = r1.shape[1]
            self.step = min(4, self.n)

        def go(self, h, src, dst, slot, d):
            k = self.base + 2 * slot + h
            return send(src, dst, rs_send.at[k], rs_recv.at[k], {self.axis: lax.rem(self.pos + 4 + d, 4)})

        def start(self, h):
            d = DIRS[h]
            self.a[h] = self.go(h, self.g.at[lax.rem(self.pos + 2, 4), h], self.r1.at[h], 0, d)
            self.c[h] = self.go(h, self.g.at[lax.rem(self.pos + 4 - d, 4), h], self.r3.at[h], 1, -d)

        def mid(self, h):
            d = DIRS[h]
            self.a[h].wait_recv()
            idx = lax.rem(self.pos + 4 + d, 4)

            def fn(j, t):
                self.m[h, t] = (self.r1[h, t].astype(F32) + self.g[idx, h, t].astype(F32)).astype(BF16)

            tiles_add(self.n, self.step, fn)
            self.b[h] = self.go(h, self.m.at[h], self.r2.at[h], 2, d)

        def end(self, h, write):
            self.c[h].wait_recv()
            self.b[h].wait_recv()

            def fn(j, t):
                v = self.r2[h, t].astype(F32) + self.r3[h, t].astype(F32) + self.g[self.pos, h, t].astype(F32)
                write(h, j, v.astype(BF16))

            tiles_add(self.n, self.step, fn)

    class Ring8:
        def __init__(self):
            self.l, self.s = {}, {}

        def g(self, h, k):
            return gz.at[lax.rem(z + 16 + k * DIRS[h], NZ), h]

        def go(self, h, src, dst, slot, d):
            k = 24 + 2 * slot + h
            return send(src, dst, rs_send.at[k], rs_recv.at[k], {"sp_0": lax.rem(z + NZ + d, NZ)})

        def start(self, h):
            d = DIRS[h]
            self.l[h] = self.go(h, self.g(h, 4), rlz.at[h, 0], 0, d)
            self.s[h] = self.go(h, self.g(h, -3), rsz.at[h, 0], 4, -d)

        def add(self, h, r, q, m, k):
            own = self.g(h, k)

            def fn(j, t):
                m[h, q, t] = (r[h, q, t].astype(F32) + own[t].astype(F32)).astype(BF16)

            tiles_add(8, 4, fn)

        def long(self, h, r):
            self.l[h].wait_recv()
            self.add(h, rlz, r - 1, mlz, 4 - r)
            self.l[h] = self.go(h, mlz.at[h, r - 1], rlz.at[h, r], r, DIRS[h])

        def short(self, h, r):
            self.s[h].wait_recv()
            self.add(h, rsz, r - 1, msz, r - 3)
            self.s[h] = self.go(h, msz.at[h, r - 1], rsz.at[h, r], 4 + r, -DIRS[h])

        def end(self, h):
            self.l[h].wait_recv()
            self.s[h].wait_recv()
            for yl in range(2):
                t = slice(4 * yl, 4 * yl + 4)
                v = rlz[h, 3, t].astype(F32) + rsz[h, 2, t].astype(F32) + gz[z, h, t].astype(F32)
                v = v.astype(BF16)
                hz[2 * h + yl, 0] = v[0:2]
                hz[2 * h + yl, 1] = v[2:4]

    rx = Ring4(gx, r1x, r2x, r3x, mx, "sp_2", x, 0)
    ry = Ring4(gy, r1y, r2y, r3y, my, "sp_1", y, 6)
    rz = Ring8()
    qx = Ring4(hx, s1x, s2x, s3x, m2x, "sp_1", y, 12)
    qy = Ring4(hy, s1y, s2y, s3y, m2y, "sp_2", x, 18)
    qz = Ring4(hz, s1z, s2z, s3z, m2z, "sp_1", y, 38)

    for hf in range(2):

        @pl.loop(0, HZ)
        def _(zq, hf=hf):
            partial(zq + hf * HZ, hf, zq)

        rx.start(hf)
        ry.start(hf)
    for hf in range(2):
        rz.start(hf)

    c_weight.wait()
    NB = 256

    @pl.loop(0, chans // NB)
    def _(n):
        cs = pl.ds(pl.multiple_of(n * NB, NB), NB)
        sc_v[:, cs] = jnp.dot(og_v[...], weight_v[:, cs], preferred_element_type=F32)

    zero = jnp.zeros((8, LANES), F32)

    def norm_pass(i, carry):
        rs = pl.ds(i * SB, SB)
        cen, inv = cen_b[rs, :], inv_b[rs, :]
        r_sum = jnp.zeros((SB, LANES), F32)
        r_dot = jnp.zeros((SB, LANES), F32)
        new = []
        for g in range(groups):
            n = sc_v[rs, cols(g)] * fac_v[rs, cols(g)]
            xc = (out_v[rs, cols(g)].astype(F32) - cen) * inv
            nx = n * xc
            new.append(carry[2 * g] + jnp.sum(nx.reshape(SB // 8, 8, LANES), axis=0))
            new.append(carry[2 * g + 1] + jnp.sum(n.reshape(SB // 8, 8, LANES), axis=0))
            sc = n * gain_v[g : g + 1, :]
            r_sum = r_sum + sc
            r_dot = r_dot + sc * xc
            sc_v[rs, cols(g)] = sc
        sum_b[rs, :] = r_sum
        dot_b[rs, :] = r_dot
        return tuple(new)

    sums = lax.fori_loop(0, rows // SB, norm_pass, (zero,) * (2 * groups))
    for i in range(blocks):
        st_a[1, i : i + 1, :] = jnp.sum(sum_b[blk(i), :].T, axis=0, keepdims=True)
        st_a[1, blocks + i : blocks + i + 1, :] = jnp.sum(dot_b[blk(i), :].T, axis=0, keepdims=True)
    c_st2 = send(st_a.at[1], st_b.at[1], st_sem.at[2], st_sem.at[3], other)

    def put_row(g, j, row):
        red[(g * AUX + j) // 8, j % 8 : j % 8 + 1, :] = row

    for g in range(groups):
        put_row(g, taps_n, jnp.sum(sums[2 * g], axis=0, keepdims=True))
        put_row(g, taps_n + 1, jnp.sum(sums[2 * g + 1], axis=0, keepdims=True))
        for j in range(taps_n + 2, AUX):
            put_row(g, j, jnp.zeros((1, LANES), F32))
    for t in range(groups * AUX // 8, red.shape[0]):
        red[t] = zero

    for h in range(2):
        rx.mid(h) if h == 0 else None
        ry.mid(h) if h == 0 else None
        rz.long(h, 1)
    c_st2.wait_recv()

    both = (st_a[1] + st_b[1]) * (1.0 / chan_total)
    spread(sum_b, both[0:blocks])
    spread(dot_b, both[blocks : 2 * blocks])

    @pl.loop(0, rows // SB)
    def _(i):
        rs = pl.ds(i * SB, SB)
        cen, inv = cen_b[rs, :], inv_b[rs, :]
        gs, gd = sum_b[rs, :], dot_b[rs, :]
        for g in range(groups):
            xc = (out_v[rs, cols(g)].astype(F32) - cen) * inv
            hg[g, rs, :] = inv * (sc_v[rs, cols(g)] - gs - xc * gd)

    c_back = send(
        hg.at[:, pl.ds(0, HALO), :], hg.at[:, pl.ds(rows, HALO), :],
        halo_sem.at[2], halo_sem.at[3], prv,
    )
    c_halo.wait_recv()

    @pl.when(place == 0)
    def _():
        gt[:, 0:HALO, :] = jnp.zeros((groups, HALO, LANES), F32)

    UB = 8

    def taps_part(lo, hi):
        @pl.loop(lo, hi)
        def _(g):
            def step(t, acc):
                base = pl.multiple_of(t * (8 * UB), 8 * UB)
                hs = [hg[g, pl.ds(base + 8 * b, 8), :] for b in range(UB)]
                acc = list(acc)
                for o in range(taps_n + 8 * (UB - 1)):
                    v = gt[g, pl.ds(base + (HALO - reach + o), 8), :]
                    for b in range(UB):
                        if 0 <= o - 8 * b < taps_n:
                            acc[o - 8 * b] = acc[o - 8 * b] + hs[b] * v
                return tuple(acc)

            acc = lax.fori_loop(0, rows // (8 * UB), step, (zero,) * taps_n)
            for j in range(taps_n):
                red[g * (AUX // 8) + j // 8, j % 8 : j % 8 + 1, :] = jnp.sum(
                    acc[j], axis=0, keepdims=True
                )

    TB = 8 * UB

    def gated_part(lo, hi):
        @pl.loop(lo, hi)
        def _(g):
            weights = [jnp.broadcast_to(tapsf[g, j : j + 1, :], (8, LANES)) for j in range(taps_n)]
            cs = pl.ds(pl.multiple_of(g * LANES, LANES), LANES)

            @pl.loop(0, rows // TB)
            def _(t):
                base = pl.multiple_of(t * TB, TB)
                parts = [None] * UB
                for o in range(taps_n + TB - 8):
                    v = hg[g, pl.ds(base + o, 8), :]
                    for b in range(UB):
                        j = 8 * b + reach - o
                        if 0 <= j < taps_n:
                            term = weights[j] * v
                            parts[b] = term if parts[b] is None else parts[b] + term
                gg = jnp.concatenate(parts, axis=0)
                rs = pl.ds(base, TB)
                sg = sigmoid(gate_v[rs, cs].astype(F32))
                val = value_v[rs, cs].astype(F32)
                gs = gg * sg
                gv_v[rs, cs] = gs.astype(BF16)
                gg_v[rs, cs] = (gs * val * (1.0 - sg)).astype(BF16)

    taps_part(0, 2)
    for h in range(2):
        rz.short(h, 1)
    rx.mid(1)
    ry.mid(1)
    taps_part(2, 4)
    for h in range(2):
        rz.long(h, 2)
    taps_part(4, groups)

    ar_a = []
    for k in range(1, PLANE):
        ar_a.append(send(
            red.at[pl.ds(2 * plane_pos[k - 1], 2)], red_r.at[k - 1],
            ar_send.at[k - 1], ar_recv.at[k - 1], plane_dev[k - 1],
        ))
    for h in range(2):
        rz.short(h, 2)
    c_back.wait_recv()

    @pl.when(place == last - 1)
    def _():
        hg[:, rows : rows + HALO, :] = jnp.zeros((groups, HALO, LANES), F32)

    gated_part(0, 1)
    for h in range(2):
        rz.long(h, 3)

    def to_hx(h, j, v):
        hx[j, h] = v

    def to_hy(h, j, v):
        hy[j, h] = v

    gated_part(1, 2)
    for h in range(2):
        rx.end(h, to_hx)
        qx.start(h) if h else None
        ry.end(h, to_hy)
    qx.start(0)
    qy.start(1)
    qy.start(0)

    gated_part(2, 4)
    for c in ar_a:
        c.wait_recv()
    mine = red[pl.ds(2 * p_me, 2)]
    for k in range(PLANE - 1):
        mine = mine + red_r[k]
    zred[z] = mine
    ar_b = []
    for k in range(1, NZ):
        ar_b.append(send(
            zred.at[z], zred.at[z], ar_send.at[PLANE + k], ar_recv.at[PLANE + k], z_dev[k - 1],
        ))

    gated_part(4, 5)
    for h in range(2):
        qx.mid(h)
        qy.mid(h)
    gated_part(5, groups)
    for h in range(2):
        rz.end(h)
    for h in range(2):
        qz.start(h)

    def to_e(e, n):
        def write(h, j, v):
            e[h * n : (h + 1) * n] = v

        return write

    zs = []
    for c, (q, e, zr) in enumerate(((qx, ex, zx), (qy, ey, zy))):
        for h in range(2):
            q.end(h, to_e(e, HZ))
        for k in range(1, NZ):
            zs.append(send(
                e.at[z_pos[k - 1]], zr.at[k - 1],
                z_send.at[c * NZ + k], z_recv.at[c * NZ + k], z_dev[k - 1],
            ))

    for c in ar_b:
        c.wait_recv()
    total = zred[0]
    for k in range(1, NZ):
        total = total + zred[k]
    ag[pl.ds(2 * p_me, 2)] = total
    ar_c = []
    for k in range(1, PLANE):
        ar_c.append(send(
            ag.at[pl.ds(2 * p_me, 2)], ag.at[pl.ds(2 * p_me, 2)],
            ar_send.at[PLANE + NZ + k], ar_recv.at[PLANE + NZ + k], plane_dev[k - 1],
        ))

    for h in range(2):
        qz.mid(h)
    for h in range(2):
        qz.end(h, to_e(ez, 2))
    xs = []
    for k in range(1, NX):
        xs.append(send(
            ez.at[x_pos[k - 1]], xz.at[k - 1],
            z_send.at[2 * NZ + k], z_recv.at[2 * NZ + k], x_dev[k - 1],
        ))

    for c in ar_c:
        c.wait_recv()
    for g in range(groups):
        for u in range(AUX // 8):
            tile = ag[g * (AUX // 8) + u]
            if u < taps_n // 8:
                gtaps_o[u * 8 : u * 8 + 8, cols(g)] = tile
            elif u == taps_n // 8:
                gtaps_o[u * 8 : taps_n, cols(g)] = tile[0 : taps_n - u * 8]
        for j, o in ((taps_n, ggain_o), (taps_n + 1, gshift_o)):
            o[g : g + 1, :] = ag[(g * AUX + j) // 8, j % 8 : j % 8 + 1, :]

    def last_sum(c, e, pos, r, copies):
        for k in copies:
            k.wait_recv()
        t = e[pos].astype(F32)
        for k in range(r.shape[0]):
            t = t + r[k].astype(F32)
        gproj_o[:, c * third : (c + 1) * third] = t

    last_sum(0, ex, z, zx, zs[: NZ - 1])
    last_sum(1, ey, z, zy, zs[NZ - 1 :])
    last_sum(2, ez, x, xz, xs)

    for c in sent:
        c.wait_send()


def put_kernel(*refs):
    n = len(refs) // 2
    sem = refs[-1]
    copies = [pltpu.make_async_copy(refs[i], refs[n + i], sem.at[i]) for i in range(n)]
    for c in copies:
        c.start()
    for c in copies:
        c.wait()


def local(conv_value, conv_gate, conv_out, conv_taps, norm_gain, norm_shift, proj_weight, out_grad):
    rows, chans = conv_value.shape
    taps_n = conv_taps.shape[0]
    d_model = proj_weight.shape[0]
    groups = chans // LANES
    third = chans // 3
    hbm_s = pl.BlockSpec(memory_space=pltpu.HBM)
    vm_s = pl.BlockSpec(memory_space=pltpu.VMEM)
    V = pltpu.VMEM
    DMA = pltpu.SemaphoreType.DMA

    def color():
        unit, small = (2, 16, 16, third), (2, 4, 16, third)
        return [
            V((4, 2, 16, 16, third), BF16),
            V(unit, BF16), V(unit, BF16), V(unit, BF16), V(unit, BF16),
            V((4, 2, 4, 16, third), BF16),
            V(small, BF16), V(small, BF16), V(small, BF16), V(small, BF16),
            V((8, 16, third), BF16),
            V((7, 16, third), BF16),
        ]

    tiny = (2, 2, 16, third)
    scratch = [
        V((rows, chans), BF16), V((rows, chans), BF16), V((rows, chans), BF16),
        V((taps_n, chans), BF16), V((groups, LANES), F32), V((groups, LANES), F32),
        V((d_model, chans), BF16), V((rows, d_model), BF16), DMA((8,)),
        V((2, 8, LANES), F32), V((2, 8, LANES), F32),
        *[V((rows, LANES), F32)] * 4,
        V((rows, chans), BF16), V((rows, chans), F32), V((rows, chans), F32),
        V((groups, rows + HALO, LANES), F32), V((groups, rows + HALO, LANES), F32),
        V((groups, 32, LANES), F32),
        *color(), *color(),
        V((8, 2, 8, 16, third), BF16),
        V((2, 4, 8, 16, third), BF16), V((2, 3, 8, 16, third), BF16),
        V((2, 3, 8, 16, third), BF16), V((2, 2, 8, 16, third), BF16),
        V((4, 2, 2, 16, third), BF16),
        V(tiny, BF16), V(tiny, BF16), V(tiny, BF16), V(tiny, BF16),
        V((4, 16, third), BF16), V((3, 16, third), BF16),
        V((32, 8, LANES), F32), V((PLANE - 1, 2, 8, LANES), F32), V((NZ, 2, 8, LANES), F32),
        V((32, 8, LANES), F32),
        DMA((4,)), DMA((4,)), DMA((44,)), DMA((44,)), DMA((2 * NZ + NX,)), DMA((2 * NZ + NX,)),
        DMA((2 * PLANE + NZ,)), DMA((2 * PLANE + NZ,)),
    ]
    S = jax.ShapeDtypeStruct
    shapes = (
        S((rows, chans), BF16), S((rows, chans), BF16), S((taps_n, chans), F32),
        S((groups, LANES), F32), S((groups, LANES), F32), S((16, chans), F32),
    )
    held = pl.pallas_call(
        kernel,
        name="conv_backward",
        out_shape=shapes,
        in_specs=[hbm_s] * 8,
        out_specs=(vm_s,) * 6,
        scratch_shapes=scratch,
        compiler_params=pltpu.CompilerParams(
            collective_id=0, has_side_effects=True, vmem_limit_bytes=VMEM_LIMIT
        ),
    )(*(
        pltpu.with_memory_space_constraint(a, pltpu.HBM)
        for a in (
            conv_value, conv_gate, conv_out, conv_taps,
            norm_gain.reshape(groups, LANES), norm_shift.reshape(groups, LANES), proj_weight, out_grad,
        )
    ))
    gv, gg, gtaps, ggain, gshift, gproj = pl.pallas_call(
        put_kernel,
        name="put_outputs",
        out_shape=shapes,
        in_specs=[vm_s] * len(shapes),
        out_specs=(hbm_s,) * len(shapes),
        scratch_shapes=[DMA((len(shapes),))],
        compiler_params=pltpu.CompilerParams(vmem_limit_bytes=1024 * 1024),
    )(*held)
    return gv, gg, gtaps, ggain.reshape(chans), gshift.reshape(chans), gproj


def solution(mesh):
    split = Mesh(mesh.devices.reshape(8, 4, 4, mesh.shape["tp"]), (*SP, "tp"))
    placed = (
        P(SP, "tp"), P(SP, "tp"), P(SP, "tp"), P(None, "tp"),
        P("tp"), P("tp"), P(None, "tp"), P(SP, None),
    )
    return jax.shard_map(
        local,
        mesh=split,
        in_specs=placed,
        out_specs=(P(SP, "tp"), P(SP, "tp"), P(None, "tp"), P("tp"), P("tp"), P(SP, "tp")),
        check_vma=False,
    )
```

```python
import jax
import jax.numpy as jnp
from jax import lax
from jax.experimental import pallas as pl
from jax.experimental.pallas import tpu as pltpu
from jax.sharding import Mesh
from jax.sharding import PartitionSpec as P

SP = ("sp_0", "sp_1", "sp_2")
MESH = pl.DeviceIdType.MESH
F32, BF16 = jnp.float32, jnp.bfloat16

norm_eps = 1e-05
LANES = 128
HALO = 32
AUX = 40
NX = NY = 4
NZ = 8
PLANE = NX * NY
VMEM_LIMIT = 32 * 1024 * 1024


def sigmoid(v):
    return 0.5 + 0.5 * jnp.tanh(0.5 * v)


def kernel(
    value_h, gate_h, out_h, taps_h, gain_h, shift_h, weight_h, og_h,
    gv_v, gg_v, gtaps_o, ggain_o, gshift_o, gproj_o,
    value_v, gate_v, out_v, taps_v, gain_v, shift_v, weight_v, og_v, in_sem,
    st_a, st_b, cen_b, inv_b, sum_b, dot_b, act_v, fac_v, sc_v, hg, gt, tapsf,
    gx, r_x, mx, hx, s_x, m2x, ex, zx,
    gy, r_y, my, hy, s_y, m2y, ey, zy,
    gz, r_z, mz, hz, pz,
    red, red_r, zred, ag,
    st_sem, halo_sem, rs_send, rs_recv, z_send, z_recv, ar_send, ar_recv,
):
    rows, chans = value_v.shape
    groups = chans // LANES
    taps_n = taps_v.shape[0]
    reach = taps_n - 1
    chan_total = 2.0 * chans
    z, y, x = (lax.axis_index(a) for a in SP)
    core = lax.axis_index("tp")
    place = (z * NY + y) * NX + x
    last = NZ * PLANE
    blocks = rows // LANES

    def at_place(s):
        return {"sp_0": s // PLANE, "sp_1": lax.rem(s // NX, NY), "sp_2": lax.rem(s, NX)}

    nxt = at_place(lax.rem(place + 1, last))
    prv = at_place(lax.rem(place + last - 1, last))
    other = {"tp": 1 - core}

    def load(i, src, dst):
        c = pltpu.make_async_copy(src, dst, in_sem.at[i])
        c.start()
        return c

    def send(src, dst, ss, rs, dev):
        c = pltpu.make_async_remote_copy(
            src_ref=src, dst_ref=dst, send_sem=ss, recv_sem=rs, device_id=dev, device_id_type=MESH
        )
        c.start()
        return c

    def total(ref, ss, rs):
        return pltpu.make_async_remote_copy(
            src_ref=ref, dst_ref=ref, send_sem=ss, recv_sem=rs, device_id=other, device_id_type=MESH
        )

    c_out = load(0, out_h, out_v)
    c_gain = load(1, gain_h, gain_v)
    c_shift = load(2, shift_h, shift_v)
    c_taps = load(3, taps_h, taps_v)
    c_gate = load(4, gate_h, gate_v)
    c_value = load(5, value_h, value_v)

    barrier = pltpu.get_barrier_semaphore()
    p_me = y * NX + x
    plane_dev = []
    plane_pos = []
    for k in range(1, PLANE):
        p = lax.rem(p_me + k, PLANE)
        plane_pos.append(p)
        plane_dev.append({"sp_1": p // NX, "sp_2": lax.rem(p, NX)})
    z_pos = [lax.rem(z + k, NZ) for k in range(1, NZ)]
    z_dev = [{"sp_0": p} for p in z_pos]
    partners = [other, nxt, prv] + plane_dev + z_dev
    for dev in partners:
        pl.semaphore_signal(barrier, inc=1, device_id=dev, device_id_type=MESH)

    c_out.wait()
    c_og = load(6, og_h, og_v)

    def cols(g):
        return slice(g * LANES, (g + 1) * LANES)

    def blk(i):
        return slice(i * LANES, (i + 1) * LANES)

    eye = lax.broadcasted_iota(jnp.int32, (LANES, LANES), 0) == lax.broadcasted_iota(
        jnp.int32, (LANES, LANES), 1
    )
    for i in range(blocks):
        part = out_v[blk(i), cols(0)].astype(F32)
        for g in range(1, groups):
            part = part + out_v[blk(i), cols(g)].astype(F32)
        s = jnp.sum(part, axis=1, keepdims=True)
        m = s * (1.0 / chans)
        d = out_v[blk(i), cols(0)].astype(F32) - m
        sq = d * d
        for g in range(1, groups):
            d = out_v[blk(i), cols(g)].astype(F32) - m
            sq = sq + d * d
        st_a[0, i : i + 1, :] = jnp.sum(jnp.where(eye, s, 0.0), axis=0, keepdims=True)
        st_a[0, blocks + i : blocks + i + 1, :] = jnp.sum(sq.T, axis=0, keepdims=True)

    pl.semaphore_wait(barrier, len(partners))
    c_st1 = send(st_a.at[0], st_b.at[0], st_sem.at[0], st_sem.at[1], other)

    SB = 64
    c_gate.wait()
    c_value.wait()
    c_weight = load(7, weight_h, weight_v)

    @pl.loop(0, rows // SB)
    def _(i):
        rs = pl.ds(i * SB, SB)
        for g in range(groups):
            gated = value_v[rs, cols(g)].astype(F32) * sigmoid(gate_v[rs, cols(g)].astype(F32))
            gt[g, pl.ds(HALO + i * SB, SB), :] = gated.astype(BF16).astype(F32)

    c_gain.wait()
    c_shift.wait()
    c_taps.wait()
    for g in range(groups):
        tapsf[g, 0:taps_n, :] = taps_v[:, cols(g)].astype(F32)
    c_halo = send(
        gt.at[:, pl.ds(rows, HALO), :], gt.at[:, pl.ds(0, HALO), :],
        halo_sem.at[0], halo_sem.at[1], nxt,
    )
    c_st1.wait_recv()

    def spread(dst, src):
        for i in range(blocks):
            dst[blk(i), :] = jnp.broadcast_to(src[i : i + 1, :], (LANES, LANES)).T

    own, peer = st_a[0], st_b[0]
    s0, m0 = own[0:blocks], own[blocks : 2 * blocks]
    s1, m1 = peer[0:blocks], peer[blocks : 2 * blocks]
    ds = s0 - s1
    var = (m0 + m1 + ds * ds * (1.0 / chan_total)) * (1.0 / chan_total)
    spread(cen_b, (s0 + s1) * (1.0 / chan_total))
    spread(inv_b, lax.rsqrt(var + norm_eps))

    @pl.loop(0, rows // SB)
    def _(i):
        rs = pl.ds(i * SB, SB)
        cen, inv = cen_b[rs, :], inv_b[rs, :]
        for g in range(groups):
            sh = (out_v[rs, cols(g)].astype(F32) - cen) * inv * gain_v[g : g + 1, :] + shift_v[g : g + 1, :]
            sg = sigmoid(sh)
            act_v[rs, cols(g)] = (sh * sg).astype(BF16)
            fac_v[rs, cols(g)] = sg * (1.0 + sh * (1.0 - sg))

    c_og.wait()
    zb = PLANE * 16
    third = chans // 3
    HZ = NZ // 2

    ZM = 4

    def partial(hf):
        m = ZM * zb
        lhs = og_v[:, hf * m : (hf + 1) * m]
        part = lax.dot_general(
            lhs, act_v[...], (((0,), (0,)), ((), ())), preferred_element_type=F32
        ).astype(BF16)
        for zq in range(ZM):
            for yy in range(NY):
                for xx in range(NX):
                    r0 = zq * zb + (yy * NX + xx) * 16
                    gx[xx, hf, yy * 4 + zq] = part[r0 : r0 + 16, 0:third]
                    gy[yy, hf, xx * 4 + zq] = part[r0 : r0 + 16, third : 2 * third]
                    gz[hf * ZM + zq, yy // 2, (yy % 2) * 4 + xx] = part[r0 : r0 + 16, 2 * third :]

    DIRS = (1, -1)

    def tiles_add(n, step, fn):
        @pl.loop(0, n // step)
        def _(j):
            fn(j, pl.ds(j * step, step))

    class Ring4:
        def __init__(self, g, r, m, axis, pos, base, sem):
            self.g, self.r, self.m = g, r, m
            self.axis, self.pos, self.base, self.sem = axis, pos, base, sem
            self.c = {}
            self.n = r.shape[2]
            self.step = min(4, self.n)

        def go(self, h, src, slot, d):
            self.c[slot, h] = send(
                src, self.r.at[slot, h], rs_send.at[self.sem], rs_recv.at[self.base + 2 * slot + h],
                {self.axis: lax.rem(self.pos + 4 + d, 4)},
            )

        def start(self, h):
            d = DIRS[h]
            self.go(h, self.g.at[lax.rem(self.pos + 2, 4), h], 0, d)
            self.go(h, self.g.at[lax.rem(self.pos + 4 - d, 4), h], 1, -d)

        def mid(self, h):
            d = DIRS[h]
            self.c[0, h].wait_recv()
            idx = lax.rem(self.pos + 4 + d, 4)

            def fn(j, t):
                self.m[h, t] = (self.r[0, h, t].astype(F32) + self.g[idx, h, t].astype(F32)).astype(BF16)

            tiles_add(self.n, self.step, fn)
            self.go(h, self.m.at[h], 2, d)

        def end(self, h, write):
            self.c[1, h].wait_recv()
            self.c[2, h].wait_recv()

            def fn(j, t):
                v = self.r[1, h, t].astype(F32) + self.r[2, h, t].astype(F32) + self.g[self.pos, h, t].astype(F32)
                write(h, j, v.astype(BF16))

            tiles_add(self.n, self.step, fn)

        def drain(self):
            total(self.r, rs_send.at[self.sem], rs_recv.at[self.base]).wait_send()

    class Ring8:
        def __init__(self, base, sem):
            self.base, self.sem = base, sem
            self.c = {}

        def g(self, h, k):
            return gz.at[lax.rem(z + 16 + k * DIRS[h], NZ), h]

        def go(self, h, src, slot, d):
            self.c[slot, h] = send(
                src, r_z.at[slot, h], rs_send.at[self.sem], rs_recv.at[self.base + 2 * slot + h],
                {"sp_0": lax.rem(z + NZ + d, NZ)},
            )

        def start(self, h):
            d = DIRS[h]
            self.go(h, self.g(h, 4), 0, d)
            self.go(h, self.g(h, -3), 4, -d)

        def hop(self, h, slot, k, d):
            self.c[slot, h].wait_recv()
            own = self.g(h, k)
            q = slot if slot < 4 else slot - 1

            def fn(j, t):
                mz[q, h, t] = (r_z[slot, h, t].astype(F32) + own[t].astype(F32)).astype(BF16)

            tiles_add(8, 4, fn)
            self.go(h, mz.at[q, h], slot + 1, d)

        def long(self, h, r):
            self.hop(h, r - 1, 4 - r, DIRS[h])

        def short(self, h, r):
            self.hop(h, 3 + r, r - 3, -DIRS[h])

        def end(self, h):
            self.c[3, h].wait_recv()
            self.c[6, h].wait_recv()

            def fn(j, t):
                v = r_z[3, h, t].astype(F32) + r_z[6, h, t].astype(F32) + gz[z, h, t].astype(F32)
                hz[pl.ds(h * 8 + j * 4, 4)] = v.astype(BF16)

            tiles_add(8, 4, fn)

        def drain(self):
            total(r_z, rs_send.at[self.sem], rs_recv.at[self.base]).wait_send()

    rx = Ring4(gx, r_x, mx, "sp_2", x, 0, 0)
    ry = Ring4(gy, r_y, my, "sp_1", y, 6, 1)
    qx = Ring4(hx, s_x, m2x, "sp_1", y, 12, 2)
    qy = Ring4(hy, s_y, m2y, "sp_2", x, 18, 3)
    rz = Ring8(24, 4)

    for hf in range(2):
        partial(hf)
        rx.start(hf)
        ry.start(hf)
    for hf in range(2):
        rz.start(hf)

    c_weight.wait()
    NB = 256

    @pl.loop(0, chans // NB)
    def _(n):
        cs = pl.ds(pl.multiple_of(n * NB, NB), NB)
        sc_v[:, cs] = jnp.dot(og_v[...], weight_v[:, cs], preferred_element_type=F32)

    zero = jnp.zeros((8, LANES), F32)

    def norm_pass(i, carry):
        rs = pl.ds(i * SB, SB)
        cen, inv = cen_b[rs, :], inv_b[rs, :]
        r_sum = jnp.zeros((SB, LANES), F32)
        r_dot = jnp.zeros((SB, LANES), F32)
        new = []
        for g in range(groups):
            n = sc_v[rs, cols(g)] * fac_v[rs, cols(g)]
            xc = (out_v[rs, cols(g)].astype(F32) - cen) * inv
            nx = n * xc
            new.append(carry[2 * g] + jnp.sum(nx.reshape(SB // 8, 8, LANES), axis=0))
            new.append(carry[2 * g + 1] + jnp.sum(n.reshape(SB // 8, 8, LANES), axis=0))
            sc = n * gain_v[g : g + 1, :]
            r_sum = r_sum + sc
            r_dot = r_dot + sc * xc
            sc_v[rs, cols(g)] = sc
        sum_b[rs, :] = r_sum
        dot_b[rs, :] = r_dot
        return tuple(new)

    sums = lax.fori_loop(0, rows // SB, norm_pass, (zero,) * (2 * groups))
    for i in range(blocks):
        st_a[1, i : i + 1, :] = jnp.sum(sum_b[blk(i), :].T, axis=0, keepdims=True)
        st_a[1, blocks + i : blocks + i + 1, :] = jnp.sum(dot_b[blk(i), :].T, axis=0, keepdims=True)
    c_st2 = send(st_a.at[1], st_b.at[1], st_sem.at[2], st_sem.at[3], other)

    def put_row(g, j, row):
        red[(g * AUX + j) // 8, j % 8 : j % 8 + 1, :] = row

    for g in range(groups):
        put_row(g, taps_n, jnp.sum(sums[2 * g], axis=0, keepdims=True))
        put_row(g, taps_n + 1, jnp.sum(sums[2 * g + 1], axis=0, keepdims=True))
        for j in range(taps_n + 2, AUX):
            put_row(g, j, jnp.zeros((1, LANES), F32))
    for t in range(groups * AUX // 8, red.shape[0]):
        red[t] = zero

    c_st2.wait_recv()

    both = (st_a[1] + st_b[1]) * (1.0 / chan_total)
    spread(sum_b, both[0:blocks])
    spread(dot_b, both[blocks : 2 * blocks])

    @pl.loop(0, rows // SB)
    def _(i):
        rs = pl.ds(i * SB, SB)
        cen, inv = cen_b[rs, :], inv_b[rs, :]
        gs, gd = sum_b[rs, :], dot_b[rs, :]
        for g in range(groups):
            xc = (out_v[rs, cols(g)].astype(F32) - cen) * inv
            hg[g, rs, :] = inv * (sc_v[rs, cols(g)] - gs - xc * gd)

    c_back = send(
        hg.at[:, pl.ds(0, HALO), :], hg.at[:, pl.ds(rows, HALO), :],
        halo_sem.at[2], halo_sem.at[3], prv,
    )
    rx.mid(0)
    ry.mid(0)
    for h in range(2):
        rz.long(h, 1)

    c_halo.wait_recv()

    @pl.when(place == 0)
    def _():
        gt[:, 0:HALO, :] = jnp.zeros((groups, HALO, LANES), F32)

    UB = 8

    def taps_part(lo, hi):
        @pl.loop(lo, hi)
        def _(g):
            def step(t, acc):
                base = pl.multiple_of(t * (8 * UB), 8 * UB)
                hs = [hg[g, pl.ds(base + 8 * b, 8), :] for b in range(UB)]
                acc = list(acc)
                for o in range(taps_n + 8 * (UB - 1)):
                    v = gt[g, pl.ds(base + (HALO - reach + o), 8), :]
                    for b in range(UB):
                        if 0 <= o - 8 * b < taps_n:
                            acc[o - 8 * b] = acc[o - 8 * b] + hs[b] * v
                return tuple(acc)

            acc = lax.fori_loop(0, rows // (8 * UB), step, (zero,) * taps_n)
            for j in range(taps_n):
                red[g * (AUX // 8) + j // 8, j % 8 : j % 8 + 1, :] = jnp.sum(
                    acc[j], axis=0, keepdims=True
                )

    TB = 8 * UB

    def gated_part(lo, hi):
        @pl.loop(lo, hi)
        def _(g):
            weights = [jnp.broadcast_to(tapsf[g, j : j + 1, :], (8, LANES)) for j in range(taps_n)]
            cs = pl.ds(pl.multiple_of(g * LANES, LANES), LANES)

            @pl.loop(0, rows // TB)
            def _(t):
                base = pl.multiple_of(t * TB, TB)
                parts = [None] * UB
                for o in range(taps_n + TB - 8):
                    v = hg[g, pl.ds(base + o, 8), :]
                    for b in range(UB):
                        j = 8 * b + reach - o
                        if 0 <= j < taps_n:
                            term = weights[j] * v
                            parts[b] = term if parts[b] is None else parts[b] + term
                gg = jnp.concatenate(parts, axis=0)
                rs = pl.ds(base, TB)
                sg = sigmoid(gate_v[rs, cs].astype(F32))
                val = value_v[rs, cs].astype(F32)
                gs = gg * sg
                gv_v[rs, cs] = gs.astype(BF16)
                gg_v[rs, cs] = (gs * val * (1.0 - sg)).astype(BF16)

    def to_hx(h, j, v):
        hx[j, h] = v

    def to_hy(h, j, v):
        hy[j, h] = v

    def to_e(e):
        def write(h, j, v):
            e[h * HZ : (h + 1) * HZ] = v

        return write

    def send_z(i, e, zr, h):
        for p in range(h * HZ, (h + 1) * HZ):

            @pl.when(z != p)
            def _(p=p):
                send(e.at[p], zr.at[z], z_send.at[i], z_recv.at[i], {"sp_0": p})

    taps_part(0, 2)
    for h in range(2):
        rz.short(h, 1)
    rx.mid(1)
    ry.mid(1)
    taps_part(2, groups)
    for k in range(1, PLANE):
        send(
            red.at[pl.ds(2 * plane_pos[k - 1], 2)], red_r.at[k - 1],
            ar_send.at[0], ar_recv.at[0], plane_dev[k - 1],
        )
    for h in range(2):
        rz.long(h, 2)
    c_back.wait_recv()

    @pl.when(place == last - 1)
    def _():
        hg[:, rows : rows + HALO, :] = jnp.zeros((groups, HALO, LANES), F32)

    gated_part(0, 1)
    rx.end(0, to_hx)
    qx.start(0)
    ry.end(0, to_hy)
    qy.start(0)
    for h in range(2):
        rz.short(h, 2)
    gated_part(1, 2)
    rx.end(1, to_hx)
    qx.start(1)
    ry.end(1, to_hy)
    qy.start(1)
    gated_part(2, 4)
    for h in range(2):
        rz.long(h, 3)
    qx.mid(0)
    qy.mid(0)
    total(red_r, ar_send.at[0], ar_recv.at[0]).wait_recv()
    mine = red[pl.ds(2 * p_me, 2)]
    for k in range(PLANE - 1):
        mine = mine + red_r[k]
    zred[z] = mine
    for k in range(1, NZ):
        send(zred.at[z], zred.at[z], ar_send.at[1], ar_recv.at[1], z_dev[k - 1])
    gated_part(4, 5)
    qx.mid(1)
    qy.mid(1)
    gated_part(5, groups)
    qx.end(0, to_e(ex))
    send_z(0, ex, zx, 0)
    qy.end(0, to_e(ey))
    send_z(1, ey, zy, 0)
    for h in range(2):
        rz.end(h)
    for k in range(1, PLANE):
        send(
            hz.at[plane_pos[k - 1]], pz.at[k - 1], z_send.at[2], z_recv.at[2], plane_dev[k - 1],
        )
    qx.end(1, to_e(ex))
    send_z(0, ex, zx, 1)
    qy.end(1, to_e(ey))
    send_z(1, ey, zy, 1)

    total(zred.at[0 : NZ - 1], ar_send.at[1], ar_recv.at[1]).wait_recv()
    tot = zred[0]
    for k in range(1, NZ):
        tot = tot + zred[k]
    ag[pl.ds(2 * p_me, 2)] = tot
    for k in range(1, PLANE):
        send(
            ag.at[pl.ds(2 * p_me, 2)], ag.at[pl.ds(2 * p_me, 2)],
            ar_send.at[2], ar_recv.at[2], plane_dev[k - 1],
        )

    total(pz, z_send.at[2], z_recv.at[2]).wait_recv()
    t = hz[p_me].astype(F32)
    for k in range(PLANE - 1):
        t = t + pz[k].astype(F32)
    gproj_o[:, 2 * third :] = t

    total(ag.at[0 : 2 * PLANE - 2], ar_send.at[2], ar_recv.at[2]).wait_recv()
    for g in range(groups):
        for u in range(AUX // 8):
            tile = ag[g * (AUX // 8) + u]
            if u < taps_n // 8:
                gtaps_o[u * 8 : u * 8 + 8, cols(g)] = tile
            elif u == taps_n // 8:
                gtaps_o[u * 8 : taps_n, cols(g)] = tile[0 : taps_n - u * 8]
        for j, o in ((taps_n, ggain_o), (taps_n + 1, gshift_o)):
            o[g : g + 1, :] = ag[(g * AUX + j) // 8, j % 8 : j % 8 + 1, :]

    for i, (e, zr) in enumerate(((ex, zx), (ey, zy))):
        total(zr.at[0 : NZ - 1], z_send.at[i], z_recv.at[i]).wait_recv()
        zr[z] = e[z]
        t = zr[0].astype(F32)
        for k in range(1, NZ):
            t = t + zr[k].astype(F32)
        gproj_o[:, i * third : (i + 1) * third] = t

    for c in (c_st1, c_st2, c_halo, c_back):
        c.wait_send()
    for q in (rx, ry, qx, qy, rz):
        q.drain()
    for i, ref in enumerate((red_r, zred.at[0 : NZ - 1], ag.at[0 : 2 * PLANE - 2])):
        total(ref, ar_send.at[i], ar_recv.at[i]).wait_send()
    for i, ref in enumerate((zx.at[0 : NZ - 1], zy.at[0 : NZ - 1], pz)):
        total(ref, z_send.at[i], z_recv.at[i]).wait_send()


def put_kernel(*refs):
    n = len(refs) // 2
    sem = refs[-1]
    copies = [pltpu.make_async_copy(refs[i], refs[n + i], sem.at[i]) for i in range(n)]
    for c in copies:
        c.start()
    for c in copies:
        c.wait()


def local(conv_value, conv_gate, conv_out, conv_taps, norm_gain, norm_shift, proj_weight, out_grad):
    rows, chans = conv_value.shape
    taps_n = conv_taps.shape[0]
    d_model = proj_weight.shape[0]
    groups = chans // LANES
    third = chans // 3
    hbm_s = pl.BlockSpec(memory_space=pltpu.HBM)
    vm_s = pl.BlockSpec(memory_space=pltpu.VMEM)
    V = pltpu.VMEM
    DMA = pltpu.SemaphoreType.DMA

    def color():
        return [
            V((4, 2, 16, 16, third), BF16), V((3, 2, 16, 16, third), BF16), V((2, 16, 16, third), BF16),
            V((4, 2, 4, 16, third), BF16), V((3, 2, 4, 16, third), BF16), V((2, 4, 16, third), BF16),
            V((NZ, 16, third), BF16), V((NZ, 16, third), BF16),
        ]

    scratch = [
        V((rows, chans), BF16), V((rows, chans), BF16), V((rows, chans), BF16),
        V((taps_n, chans), BF16), V((groups, LANES), F32), V((groups, LANES), F32),
        V((d_model, chans), BF16), V((rows, d_model), BF16), DMA((8,)),
        V((2, 8, LANES), F32), V((2, 8, LANES), F32),
        *[V((rows, LANES), F32)] * 4,
        V((rows, chans), BF16), V((rows, chans), F32), V((rows, chans), F32),
        V((groups, rows + HALO, LANES), F32), V((groups, rows + HALO, LANES), F32),
        V((groups, 32, LANES), F32),
        *color(), *color(),
        V((NZ, 2, 8, 16, third), BF16), V((7, 2, 8, 16, third), BF16), V((5, 2, 8, 16, third), BF16),
        V((PLANE, 16, third), BF16), V((PLANE - 1, 16, third), BF16),
        V((2 * PLANE, 8, LANES), F32), V((PLANE - 1, 2, 8, LANES), F32), V((NZ, 2, 8, LANES), F32),
        V((2 * PLANE, 8, LANES), F32),
        DMA((4,)), DMA((4,)), DMA((5,)), DMA((38,)), DMA((3,)), DMA((3,)), DMA((3,)), DMA((3,)),
    ]
    S = jax.ShapeDtypeStruct
    shapes = (
        S((rows, chans), BF16), S((rows, chans), BF16), S((taps_n, chans), F32),
        S((groups, LANES), F32), S((groups, LANES), F32), S((16, chans), F32),
    )
    held = pl.pallas_call(
        kernel,
        name="conv_backward",
        out_shape=shapes,
        in_specs=[hbm_s] * 8,
        out_specs=(vm_s,) * 6,
        scratch_shapes=scratch,
        compiler_params=pltpu.CompilerParams(
            collective_id=0, has_side_effects=True, vmem_limit_bytes=VMEM_LIMIT
        ),
    )(*(
        pltpu.with_memory_space_constraint(a, pltpu.HBM)
        for a in (
            conv_value, conv_gate, conv_out, conv_taps,
            norm_gain.reshape(groups, LANES), norm_shift.reshape(groups, LANES), proj_weight, out_grad,
        )
    ))
    gv, gg, gtaps, ggain, gshift, gproj = pl.pallas_call(
        put_kernel,
        name="put_outputs",
        out_shape=shapes,
        in_specs=[vm_s] * len(shapes),
        out_specs=(hbm_s,) * len(shapes),
        scratch_shapes=[DMA((len(shapes),))],
        compiler_params=pltpu.CompilerParams(vmem_limit_bytes=1024 * 1024),
    )(*held)
    return gv, gg, gtaps, ggain.reshape(chans), gshift.reshape(chans), gproj


def solution(mesh):
    split = Mesh(mesh.devices.reshape(8, 4, 4, mesh.shape["tp"]), (*SP, "tp"))
    placed = (
        P(SP, "tp"), P(SP, "tp"), P(SP, "tp"), P(None, "tp"),
        P("tp"), P("tp"), P(None, "tp"), P(SP, None),
    )
    return jax.shard_map(
        local,
        mesh=split,
        in_specs=placed,
        out_specs=(P(SP, "tp"), P(SP, "tp"), P(None, "tp"), P("tp"), P("tp"), P(SP, "tp")),
        check_vma=False,
    )
```

```python
import jax
import jax.numpy as jnp
from jax import lax
from jax.experimental import pallas as pl
from jax.experimental.pallas import tpu as pltpu
from jax.sharding import Mesh
from jax.sharding import PartitionSpec as P

SP = ("sp_0", "sp_1", "sp_2")
MESH = pl.DeviceIdType.MESH
F32, BF16 = jnp.float32, jnp.bfloat16

norm_eps = 1e-05
LANES = 128
HALO = 32
AUX = 40
NX = NY = 4
NZ = 8
PLANE = NX * NY
VMEM_LIMIT = 32 * 1024 * 1024


def sigmoid(v):
    return 0.5 + 0.5 * jnp.tanh(0.5 * v)


def kernel(
    value_h, gate_h, out_h, taps_h, gain_h, shift_h, weight_h, og_h,
    gv_v, gg_v, gtaps_o, ggain_o, gshift_o, gproj_o,
    value_v, gate_v, out_v, taps_v, gain_v, shift_v, weight_v, og_v, in_sem,
    st_a, st_b, cen_b, inv_b, sum_b, dot_b, act_v, fac_v, sc_v, hg, gt, tapsf, edge, edge_r,
    gx, r_x, mx, hx, s_x, m2x, ex, zx,
    gy, r_y, my, hy, s_y, m2y, ey, zy,
    gz, r_z, mz, hz, pz,
    red, red_r, zred, ag,
    st_sem, halo_sem, rs_send, rs_recv, z_send, z_recv, ar_send, ar_recv,
):
    rows, chans = value_v.shape
    groups = chans // LANES
    taps_n = taps_v.shape[0]
    reach = taps_n - 1
    chan_total = 2.0 * chans
    z, y, x = (lax.axis_index(a) for a in SP)
    core = lax.axis_index("tp")
    place = (z * NY + y) * NX + x
    last = NZ * PLANE
    blocks = rows // LANES
    NB = 256

    def at_place(s):
        return {"sp_0": s // PLANE, "sp_1": lax.rem(s // NX, NY), "sp_2": lax.rem(s, NX)}

    nxt = at_place(lax.rem(place + 1, last))
    prv = at_place(lax.rem(place + last - 1, last))
    other = {"tp": 1 - core}

    def load(i, src, dst):
        c = pltpu.make_async_copy(src, dst, in_sem.at[i])
        c.start()
        return c

    def send(src, dst, ss, rs, dev):
        c = pltpu.make_async_remote_copy(
            src_ref=src, dst_ref=dst, send_sem=ss, recv_sem=rs, device_id=dev, device_id_type=MESH
        )
        c.start()
        return c

    def total(ref, ss, rs):
        return pltpu.make_async_remote_copy(
            src_ref=ref, dst_ref=ref, send_sem=ss, recv_sem=rs, device_id=other, device_id_type=MESH
        )

    def blk(i):
        return slice(i * LANES, (i + 1) * LANES)

    c_out = [load(8 + i, out_h.at[blk(i)], out_v.at[blk(i)]) for i in range(blocks)]
    body, tail = slice(0, rows - HALO), slice(rows - HALO, rows)
    c_tail = [
        load(4, gate_h.at[tail], gate_v.at[tail]), load(5, value_h.at[tail], value_v.at[tail])
    ]
    c_gain = load(1, gain_h, gain_v)
    c_shift = load(2, shift_h, shift_v)
    c_taps = load(3, taps_h, taps_v)

    c_og = load(6, og_h, og_v)
    c_weight = [
        load(n, weight_h.at[:, cs], weight_v.at[:, cs])
        for n, cs in ((0, slice(0, NB)), (7, slice(NB, chans)))
    ]

    barrier = pltpu.get_barrier_semaphore()
    p_me = y * NX + x
    plane_dev = []
    plane_pos = []
    for k in range(1, PLANE):
        p = lax.rem(p_me + k, PLANE)
        plane_pos.append(p)
        plane_dev.append({"sp_1": p // NX, "sp_2": lax.rem(p, NX)})
    z_pos = [lax.rem(z + k, NZ) for k in range(1, NZ)]
    z_dev = [{"sp_0": p} for p in z_pos]
    partners = [other, nxt, prv] + plane_dev + z_dev
    for dev in partners:
        pl.semaphore_signal(barrier, inc=1, device_id=dev, device_id_type=MESH)

    c_out[0].wait()
    c_body = [
        load(12, gate_h.at[body], gate_v.at[body]), load(13, value_h.at[body], value_v.at[body])
    ]

    def cols(g):
        return slice(g * LANES, (g + 1) * LANES)

    eye = lax.broadcasted_iota(jnp.int32, (LANES, LANES), 0) == lax.broadcasted_iota(
        jnp.int32, (LANES, LANES), 1
    )
    for i in range(blocks):
        if i:
            c_out[i].wait()
        part = out_v[blk(i), cols(0)].astype(F32)
        for g in range(1, groups):
            part = part + out_v[blk(i), cols(g)].astype(F32)
        s = jnp.sum(part, axis=1, keepdims=True)
        m = s * (1.0 / chans)
        d = out_v[blk(i), cols(0)].astype(F32) - m
        sq = d * d
        for g in range(1, groups):
            d = out_v[blk(i), cols(g)].astype(F32) - m
            sq = sq + d * d
        st_a[0, i : i + 1, :] = jnp.sum(jnp.where(eye, s, 0.0), axis=0, keepdims=True)
        st_a[0, blocks + i : blocks + i + 1, :] = jnp.sum(sq.T, axis=0, keepdims=True)

    pl.semaphore_wait(barrier, len(partners))
    c_st1 = send(st_a.at[0], st_b.at[0], st_sem.at[0], st_sem.at[1], other)

    SB = 64
    def gate_rows(lo, n):
        rs = pl.ds(lo, n)
        for g in range(groups):
            gated = value_v[rs, cols(g)].astype(F32) * sigmoid(gate_v[rs, cols(g)].astype(F32))
            gt[g, pl.ds(HALO + lo, n), :] = gated.astype(BF16).astype(F32)

    for c in c_tail:
        c.wait()
    gate_rows(rows - HALO, HALO)
    c_halo = send(
        gt.at[:, pl.ds(rows, HALO), :], gt.at[:, pl.ds(0, HALO), :],
        halo_sem.at[0], halo_sem.at[1], nxt,
    )
    c_gain.wait()
    c_shift.wait()
    c_taps.wait()
    for g in range(groups):
        tapsf[g, 0:taps_n, :] = taps_v[:, cols(g)].astype(F32)
    def act_grad(n):
        cs = pl.ds(pl.multiple_of(n * NB, NB), NB)
        sc_v[:, cs] = jnp.dot(og_v[...], weight_v[:, cs], preferred_element_type=F32)

    c_og.wait()
    c_weight[0].wait()
    act_grad(0)
    c_st1.wait_recv()

    def spread(dst, src):
        for i in range(blocks):
            dst[blk(i), :] = jnp.broadcast_to(src[i : i + 1, :], (LANES, LANES)).T

    own, peer = st_a[0], st_b[0]
    s0, m0 = own[0:blocks], own[blocks : 2 * blocks]
    s1, m1 = peer[0:blocks], peer[blocks : 2 * blocks]
    ds = s0 - s1
    var = (m0 + m1 + ds * ds * (1.0 / chan_total)) * (1.0 / chan_total)
    spread(cen_b, (s0 + s1) * (1.0 / chan_total))
    spread(inv_b, lax.rsqrt(var + norm_eps))

    @pl.loop(0, rows // SB)
    def _(i):
        rs = pl.ds(i * SB, SB)
        cen, inv = cen_b[rs, :], inv_b[rs, :]
        for g in range(groups):
            sh = (out_v[rs, cols(g)].astype(F32) - cen) * inv * gain_v[g : g + 1, :] + shift_v[g : g + 1, :]
            sg = sigmoid(sh)
            act = sh * sg
            act_v[rs, cols(g)] = act.astype(BF16)
            fac_v[rs, cols(g)] = sg + act * (1.0 - sg)

    zb = PLANE * 16
    third = chans // 3
    HZ = NZ // 2

    ZM = 4

    def partial(hf):
        m = ZM * zb
        lhs = og_v[:, hf * m : (hf + 1) * m]
        part = lax.dot_general(
            lhs, act_v[...], (((0,), (0,)), ((), ())), preferred_element_type=F32
        ).astype(BF16)
        for zq in range(ZM):
            for yy in range(NY):
                for xx in range(NX):
                    r0 = zq * zb + (yy * NX + xx) * 16
                    for c in range(third // LANES):
                        piece = [
                            part[r0 : r0 + 16, i * third + c * LANES : i * third + (c + 1) * LANES]
                            for i in range(3)
                        ]
                        gx[xx, hf, yy * 4 + zq, c] = piece[0]
                        gy[yy, hf, xx * 4 + zq, c] = piece[1]
                        gz[hf * ZM + zq, yy // 2, (yy % 2) * 4 + xx, c] = piece[2]

    DIRS = (1, -1)

    def tiles_add(n, step, fn):
        @pl.loop(0, n // step)
        def _(j):
            fn(j, pl.ds(j * step, step))

    class Ring4:
        def __init__(self, g, r, m, axis, pos, base, sem):
            self.g, self.r, self.m = g, r, m
            self.axis, self.pos, self.base, self.sem = axis, pos, base, sem
            self.c = {}
            self.n = r.shape[2]
            self.step = min(4, self.n)

        def go(self, h, src, slot, d):
            self.c[slot, h] = send(
                src, self.r.at[slot, h], rs_send.at[self.sem], rs_recv.at[self.base + 2 * slot + h],
                {self.axis: lax.rem(self.pos + 4 + d, 4)},
            )

        def start(self, h):
            d = DIRS[h]
            self.go(h, self.g.at[lax.rem(self.pos + 2, 4), h], 0, d)

        def single(self, h):
            d = DIRS[h]
            self.go(h, self.g.at[lax.rem(self.pos + 4 - d, 4), h], 1, -d)

        def mid(self, h):
            d = DIRS[h]
            self.c[0, h].wait_recv()
            idx = lax.rem(self.pos + 4 + d, 4)

            def fn(j, t):
                self.m[h, t] = (self.r[0, h, t].astype(F32) + self.g[idx, h, t].astype(F32)).astype(BF16)

            tiles_add(self.n, self.step, fn)
            self.go(h, self.m.at[h], 2, d)

        def end(self, h, write):
            self.c[1, h].wait_recv()
            self.c[2, h].wait_recv()

            def fn(j, t):
                v = self.r[1, h, t].astype(F32) + self.r[2, h, t].astype(F32) + self.g[self.pos, h, t].astype(F32)
                write(h, j, v.astype(BF16))

            tiles_add(self.n, self.step, fn)

        def drain(self):
            total(self.r, rs_send.at[self.sem], rs_recv.at[self.base]).wait_send()

    class Ring8:
        def __init__(self, base, sem):
            self.base, self.sem = base, sem
            self.c = {}

        def g(self, h, k):
            return gz.at[lax.rem(z + 16 + k * DIRS[h], NZ), h]

        def go(self, h, src, slot, d):
            self.c[slot, h] = send(
                src, r_z.at[slot, h], rs_send.at[self.sem], rs_recv.at[self.base + 2 * slot + h],
                {"sp_0": lax.rem(z + NZ + d, NZ)},
            )

        def start(self, h):
            d = DIRS[h]
            self.go(h, self.g(h, 4), 0, d)
            self.go(h, self.g(h, -3), 4, -d)

        def hop(self, h, slot, k, d):
            self.c[slot, h].wait_recv()
            own = self.g(h, k)
            q = slot if slot < 4 else slot - 1

            def fn(j, t):
                mz[q, h, t] = (r_z[slot, h, t].astype(F32) + own[t].astype(F32)).astype(BF16)

            tiles_add(8, 4, fn)
            self.go(h, mz.at[q, h], slot + 1, d)

        def long(self, h, r):
            self.hop(h, r - 1, 4 - r, DIRS[h])

        def short(self, h, r):
            self.hop(h, 3 + r, r - 3, -DIRS[h])

        def end(self, h):
            self.c[3, h].wait_recv()
            self.c[6, h].wait_recv()

            def fn(j, t):
                v = r_z[3, h, t].astype(F32) + r_z[6, h, t].astype(F32) + gz[z, h, t].astype(F32)
                hz[pl.ds(h * 8 + j * 4, 4)] = v.astype(BF16)

            tiles_add(8, 4, fn)

        def drain(self):
            total(r_z, rs_send.at[self.sem], rs_recv.at[self.base]).wait_send()

    rx = Ring4(gx, r_x, mx, "sp_2", x, 0, 0)
    ry = Ring4(gy, r_y, my, "sp_1", y, 6, 1)
    qx = Ring4(hx, s_x, m2x, "sp_1", y, 12, 2)
    qy = Ring4(hy, s_y, m2y, "sp_2", x, 18, 3)
    rz = Ring8(24, 4)

    for hf in range(2):
        partial(hf)
        rx.start(hf)
        ry.start(hf)
    for hf in range(2):
        rz.start(hf)
    for hf in range(2):
        rx.single(hf)
        ry.single(hf)

    c_weight[1].wait()
    pl.loop(1, chans // NB)(act_grad)

    zero = jnp.zeros((8, LANES), F32)

    def norm_pass(i, carry):
        rs = pl.ds(i * SB, SB)
        cen, inv = cen_b[rs, :], inv_b[rs, :]
        r_sum = jnp.zeros((SB, LANES), F32)
        r_dot = jnp.zeros((SB, LANES), F32)
        new = []
        for g in range(groups):
            n = sc_v[rs, cols(g)] * fac_v[rs, cols(g)]
            xc = (out_v[rs, cols(g)].astype(F32) - cen) * inv
            nx = n * xc
            new.append(carry[2 * g] + jnp.sum(nx.reshape(SB // 8, 8, LANES), axis=0))
            new.append(carry[2 * g + 1] + jnp.sum(n.reshape(SB // 8, 8, LANES), axis=0))
            sc = n * gain_v[g : g + 1, :]
            r_sum = r_sum + sc
            r_dot = r_dot + sc * xc
            sc_v[rs, cols(g)] = sc
        sum_b[rs, :] = r_sum
        dot_b[rs, :] = r_dot
        return tuple(new)

    sums = lax.fori_loop(0, rows // SB, norm_pass, (zero,) * (2 * groups))
    for i in range(blocks):
        st_a[1, i : i + 1, :] = jnp.sum(sum_b[blk(i), :].T, axis=0, keepdims=True)
        st_a[1, blocks + i : blocks + i + 1, :] = jnp.sum(dot_b[blk(i), :].T, axis=0, keepdims=True)
    c_st2 = send(st_a.at[1], st_b.at[1], st_sem.at[2], st_sem.at[3], other)

    def put_row(g, j, row):
        red[(g * AUX + j) // 8, j % 8 : j % 8 + 1, :] = row

    for g in range(groups):
        put_row(g, taps_n, jnp.sum(sums[2 * g], axis=0, keepdims=True))
        put_row(g, taps_n + 1, jnp.sum(sums[2 * g + 1], axis=0, keepdims=True))
        for j in range(taps_n + 2, AUX):
            put_row(g, j, jnp.zeros((1, LANES), F32))
    for t in range(groups * AUX // 8, red.shape[0]):
        red[t] = zero

    for c in c_body:
        c.wait()
    GB = 96
    pl.loop(0, (rows - HALO) // GB)(lambda i: gate_rows(pl.multiple_of(i * GB, GB), GB))
    c_st2.wait_recv()

    both = (st_a[1] + st_b[1]) * (1.0 / chan_total)
    spread(sum_b, both[0:blocks])
    spread(dot_b, both[blocks : 2 * blocks])

    @pl.loop(0, rows // SB)
    def _(i):
        rs = pl.ds(i * SB, SB)
        cen, inv = cen_b[rs, :], inv_b[rs, :]
        gs, gd = sum_b[rs, :], dot_b[rs, :]
        for g in range(groups):
            xc = (out_v[rs, cols(g)].astype(F32) - cen) * inv
            hg[g, rs, :] = inv * (sc_v[rs, cols(g)] - gs - xc * gd)

    for g in range(groups):
        edge[g] = hg[g, 0:HALO, :].astype(BF16)
    rx.mid(0)
    ry.mid(0)
    for h in range(2):
        rz.long(h, 1)

    c_halo.wait_recv()

    @pl.when(place == 0)
    def _():
        gt[:, 0:HALO, :] = jnp.zeros((groups, HALO, LANES), F32)

    UB = 8
    UT = 16

    def taps_part(lo, hi):
        @pl.loop(lo, hi)
        def _(g):
            def step(t, acc):
                base = pl.multiple_of(t * (8 * UT), 8 * UT)
                hs = [hg[g, pl.ds(base + 8 * b, 8), :] for b in range(UT)]
                acc = list(acc)
                for o in range(taps_n + 8 * (UT - 1)):
                    v = gt[g, pl.ds(base + (HALO - reach + o), 8), :]
                    for b in range(UT):
                        if 0 <= o - 8 * b < taps_n:
                            acc[o - 8 * b] = acc[o - 8 * b] + hs[b] * v
                return tuple(acc)

            acc = lax.fori_loop(0, rows // (8 * UT), step, (zero,) * taps_n)
            for j in range(taps_n):
                red[g * (AUX // 8) + j // 8, j % 8 : j % 8 + 1, :] = jnp.sum(
                    acc[j], axis=0, keepdims=True
                )

    TB = 8 * UB

    def gated_part(lo, hi):
        @pl.loop(0, groups)
        def _(g):
            weights = [jnp.broadcast_to(tapsf[g, j : j + 1, :], (8, LANES)) for j in range(taps_n)]
            cs = pl.ds(pl.multiple_of(g * LANES, LANES), LANES)

            @pl.loop(lo, hi)
            def _(t):
                base = pl.multiple_of(t * TB, TB)
                parts = [None] * UB
                for o in range(taps_n + TB - 8):
                    v = hg[g, pl.ds(base + o, 8), :]
                    for b in range(UB):
                        j = 8 * b + reach - o
                        if 0 <= j < taps_n:
                            term = weights[j] * v
                            parts[b] = term if parts[b] is None else parts[b] + term
                gg = jnp.concatenate(parts, axis=0)
                rs = pl.ds(base, TB)
                sg = sigmoid(gate_v[rs, cs].astype(F32))
                val = value_v[rs, cs].astype(F32)
                gs = gg * sg
                gv_v[rs, cs] = gs.astype(BF16)
                gg_v[rs, cs] = (gs * val * (1.0 - sg)).astype(BF16)

    def to_hx(h, j, v):
        hx[j, h] = v

    def to_hy(h, j, v):
        hy[j, h] = v

    def to_e(e):
        def write(h, j, v):
            e[h * HZ : (h + 1) * HZ] = v

        return write

    def send_z(i, e, zr, h):
        for p in range(h * HZ, (h + 1) * HZ):

            @pl.when(z != p)
            def _(p=p):
                send(e.at[p], zr.at[z], z_send.at[i], z_recv.at[i], {"sp_0": p})

    taps_part(0, 1)
    rx.mid(1)
    ry.mid(1)
    c_back = send(edge, edge_r, halo_sem.at[2], halo_sem.at[3], prv)
    for h in range(2):
        rz.short(h, 1)
    taps_part(1, groups)
    for k in range(1, PLANE):
        send(
            red.at[pl.ds(2 * plane_pos[k - 1], 2)], red_r.at[k - 1],
            ar_send.at[0], ar_recv.at[0], plane_dev[k - 1],
        )
    for h in range(2):
        rz.long(h, 2)
    gated_part(0, 1)
    rx.end(0, to_hx)
    qx.start(0)
    qx.single(0)
    ry.end(0, to_hy)
    qy.start(0)
    qy.single(0)
    for h in range(2):
        rz.short(h, 2)
    gated_part(1, 2)
    rx.end(1, to_hx)
    qx.start(1)
    qx.single(1)
    ry.end(1, to_hy)
    qy.start(1)
    qy.single(1)
    gated_part(2, 5)
    for h in range(2):
        rz.long(h, 3)
    qx.mid(0)
    qy.mid(0)
    total(red_r, ar_send.at[0], ar_recv.at[0]).wait_recv()
    mine = red[pl.ds(2 * p_me, 2)]
    for k in range(PLANE - 1):
        mine = mine + red_r[k]
    zred[z] = mine
    for k in range(1, NZ):
        send(zred.at[z], zred.at[z], ar_send.at[1], ar_recv.at[1], z_dev[k - 1])
    gated_part(5, 6)
    qx.mid(1)
    qy.mid(1)
    gated_part(6, 7)
    c_back.wait_recv()
    for g in range(groups):
        hg[g, rows : rows + HALO, :] = jnp.where(place == last - 1, 0.0, edge_r[g].astype(F32))
    gated_part(7, 8)
    qx.end(0, to_e(ex))
    send_z(0, ex, zx, 0)
    qy.end(0, to_e(ey))
    send_z(1, ey, zy, 0)
    for h in range(2):
        rz.end(h)
    for k in range(1, PLANE):
        send(
            hz.at[plane_pos[k - 1]], pz.at[k - 1], z_send.at[2], z_recv.at[2], plane_dev[k - 1],
        )
    qx.end(1, to_e(ex))
    send_z(0, ex, zx, 1)
    qy.end(1, to_e(ey))
    send_z(1, ey, zy, 1)

    total(zred.at[0 : NZ - 1], ar_send.at[1], ar_recv.at[1]).wait_recv()
    tot = zred[0]
    for k in range(1, NZ):
        tot = tot + zred[k]
    ag[pl.ds(2 * p_me, 2)] = tot
    for k in range(1, PLANE):
        send(
            ag.at[pl.ds(2 * p_me, 2)], ag.at[pl.ds(2 * p_me, 2)],
            ar_send.at[2], ar_recv.at[2], plane_dev[k - 1],
        )

    total(pz, z_send.at[2], z_recv.at[2]).wait_recv()
    t = hz[p_me].astype(F32)
    for k in range(PLANE - 1):
        t = t + pz[k].astype(F32)
    def put_proj(i, t):
        for c in range(third // LANES):
            gproj_o[:, i * third + c * LANES : i * third + (c + 1) * LANES] = t[c]

    put_proj(2, t)

    total(ag.at[0 : 2 * PLANE - 2], ar_send.at[2], ar_recv.at[2]).wait_recv()
    for g in range(groups):
        for u in range(AUX // 8):
            tile = ag[g * (AUX // 8) + u]
            if u < taps_n // 8:
                gtaps_o[u * 8 : u * 8 + 8, cols(g)] = tile
            elif u == taps_n // 8:
                gtaps_o[u * 8 : taps_n, cols(g)] = tile[0 : taps_n - u * 8]
        for j, o in ((taps_n, ggain_o), (taps_n + 1, gshift_o)):
            o[g : g + 1, :] = ag[(g * AUX + j) // 8, j % 8 : j % 8 + 1, :]

    for i, (e, zr) in enumerate(((ex, zx), (ey, zy))):
        total(zr.at[0 : NZ - 1], z_send.at[i], z_recv.at[i]).wait_recv()
        zr[z] = e[z]
        t = zr[0].astype(F32)
        for k in range(1, NZ):
            t = t + zr[k].astype(F32)
        put_proj(i, t)

    for c in (c_st1, c_st2, c_halo, c_back):
        c.wait_send()
    for q in (rx, ry, qx, qy, rz):
        q.drain()
    for i, ref in enumerate((red_r, zred.at[0 : NZ - 1], ag.at[0 : 2 * PLANE - 2])):
        total(ref, ar_send.at[i], ar_recv.at[i]).wait_send()
    for i, ref in enumerate((zx.at[0 : NZ - 1], zy.at[0 : NZ - 1], pz)):
        total(ref, z_send.at[i], z_recv.at[i]).wait_send()


def put_kernel(*refs):
    n = len(refs) // 2
    sem = refs[-1]
    copies = [pltpu.make_async_copy(refs[i], refs[n + i], sem.at[i]) for i in range(n)]
    for c in copies:
        c.start()
    for c in copies:
        c.wait()


def local(conv_value, conv_gate, conv_out, conv_taps, norm_gain, norm_shift, proj_weight, out_grad):
    rows, chans = conv_value.shape
    taps_n = conv_taps.shape[0]
    d_model = proj_weight.shape[0]
    groups = chans // LANES
    third = chans // 3
    hbm_s = pl.BlockSpec(memory_space=pltpu.HBM)
    vm_s = pl.BlockSpec(memory_space=pltpu.VMEM)
    V = pltpu.VMEM
    DMA = pltpu.SemaphoreType.DMA

    def color():
        return [
            V((4, 2, 16, third // LANES, 16, LANES), BF16), V((3, 2, 16, third // LANES, 16, LANES), BF16), V((2, 16, third // LANES, 16, LANES), BF16),
            V((4, 2, 4, third // LANES, 16, LANES), BF16), V((3, 2, 4, third // LANES, 16, LANES), BF16), V((2, 4, third // LANES, 16, LANES), BF16),
            V((NZ, third // LANES, 16, LANES), BF16), V((NZ, third // LANES, 16, LANES), BF16),
        ]

    scratch = [
        V((rows, chans), BF16), V((rows, chans), BF16), V((rows, chans), BF16),
        V((taps_n, chans), BF16), V((groups, LANES), F32), V((groups, LANES), F32),
        V((d_model, chans), BF16), V((rows, d_model), BF16), DMA((14,)),
        V((2, 8, LANES), F32), V((2, 8, LANES), F32),
        *[V((rows, LANES), F32)] * 4,
        V((rows, chans), BF16), V((rows, chans), F32), V((rows, chans), F32),
        V((groups, rows + HALO, LANES), F32), V((groups, rows + HALO, LANES), F32),
        V((groups, 32, LANES), F32), V((groups, HALO, LANES), BF16), V((groups, HALO, LANES), BF16),
        *color(), *color(),
        V((NZ, 2, 8, third // LANES, 16, LANES), BF16), V((7, 2, 8, third // LANES, 16, LANES), BF16), V((5, 2, 8, third // LANES, 16, LANES), BF16),
        V((PLANE, third // LANES, 16, LANES), BF16), V((PLANE - 1, third // LANES, 16, LANES), BF16),
        V((2 * PLANE, 8, LANES), F32), V((PLANE - 1, 2, 8, LANES), F32), V((NZ, 2, 8, LANES), F32),
        V((2 * PLANE, 8, LANES), F32),
        DMA((4,)), DMA((4,)), DMA((5,)), DMA((38,)), DMA((3,)), DMA((3,)), DMA((3,)), DMA((3,)),
    ]
    S = jax.ShapeDtypeStruct
    shapes = (
        S((rows, chans), BF16), S((rows, chans), BF16), S((taps_n, chans), F32),
        S((groups, LANES), F32), S((groups, LANES), F32), S((16, chans), F32),
    )
    held = pl.pallas_call(
        kernel,
        name="conv_backward",
        out_shape=shapes,
        in_specs=[hbm_s] * 8,
        out_specs=(vm_s,) * 6,
        scratch_shapes=scratch,
        compiler_params=pltpu.CompilerParams(
            collective_id=0, has_side_effects=True, vmem_limit_bytes=VMEM_LIMIT
        ),
    )(*(
        pltpu.with_memory_space_constraint(a, pltpu.HBM)
        for a in (
            conv_value, conv_gate, conv_out, conv_taps,
            norm_gain.reshape(groups, LANES), norm_shift.reshape(groups, LANES), proj_weight, out_grad,
        )
    ))
    gv, gg, gtaps, ggain, gshift, gproj = pl.pallas_call(
        put_kernel,
        name="put_outputs",
        out_shape=shapes,
        in_specs=[vm_s] * len(shapes),
        out_specs=(hbm_s,) * len(shapes),
        scratch_shapes=[DMA((len(shapes),))],
        compiler_params=pltpu.CompilerParams(vmem_limit_bytes=1024 * 1024),
    )(*held)
    return gv, gg, gtaps, ggain.reshape(chans), gshift.reshape(chans), gproj


def solution(mesh):
    split = Mesh(mesh.devices.reshape(8, 4, 4, mesh.shape["tp"]), (*SP, "tp"))
    placed = (
        P(SP, "tp"), P(SP, "tp"), P(SP, "tp"), P(None, "tp"),
        P("tp"), P("tp"), P(None, "tp"), P(SP, None),
    )
    return jax.shard_map(
        local,
        mesh=split,
        in_specs=placed,
        out_specs=(P(SP, "tp"), P(SP, "tp"), P(None, "tp"), P("tp"), P("tp"), P(SP, "tp")),
        check_vma=False,
    )
```

```python
import jax
import jax.numpy as jnp
from jax import lax
from jax.experimental import pallas as pl
from jax.experimental.pallas import tpu as pltpu
from jax.sharding import Mesh
from jax.sharding import PartitionSpec as P

SP = ("sp_0", "sp_1", "sp_2")
MESH = pl.DeviceIdType.MESH
F32, BF16 = jnp.float32, jnp.bfloat16

norm_eps = 1e-05
LANES = 128
HALO = 32
AUX = 40
NX = NY = 4
NZ = 8
PLANE = NX * NY
VMEM_LIMIT = 32 * 1024 * 1024


def sigmoid(v):
    return 0.5 + 0.5 * jnp.tanh(0.5 * v)


def kernel(
    value_h, gate_h, out_h, taps_h, gain_h, shift_h, weight_h, og_h,
    gv_v, gg_v, gtaps_o, ggain_o, gshift_o, gproj_o,
    value_v, gate_v, out_v, taps_v, gain_v, shift_v, weight_v, og_v, in_sem,
    st_a, st_b, cen_b, inv_b, sum_b, dot_b, act_v, fac_v, sc_v, hg, gt, tapsf, edge, edge_r,
    gx, r_x, mx, hx, s_x, m2x, ex, zx,
    gy, r_y, my, hy, s_y, m2y, ey, zy,
    gz, r_z, mz, hz, pz,
    red, red_r, zred, ag,
    st_sem, halo_sem, rs_send, rs_recv, z_send, z_recv, ar_send, ar_recv,
):
    rows, chans = value_v.shape
    groups = chans // LANES
    taps_n = taps_v.shape[0]
    reach = taps_n - 1
    chan_total = 2.0 * chans
    z, y, x = (lax.axis_index(a) for a in SP)
    core = lax.axis_index("tp")
    place = (z * NY + y) * NX + x
    last = NZ * PLANE
    blocks = rows // LANES
    NB = 256

    def at_place(s):
        return {"sp_0": s // PLANE, "sp_1": lax.rem(s // NX, NY), "sp_2": lax.rem(s, NX)}

    nxt = at_place(lax.rem(place + 1, last))
    prv = at_place(lax.rem(place + last - 1, last))
    other = {"tp": 1 - core}

    def load(i, src, dst):
        c = pltpu.make_async_copy(src, dst, in_sem.at[i])
        c.start()
        return c

    def send(src, dst, ss, rs, dev):
        c = pltpu.make_async_remote_copy(
            src_ref=src, dst_ref=dst, send_sem=ss, recv_sem=rs, device_id=dev, device_id_type=MESH
        )
        c.start()
        return c

    def total(ref, ss, rs):
        return pltpu.make_async_remote_copy(
            src_ref=ref, dst_ref=ref, send_sem=ss, recv_sem=rs, device_id=other, device_id_type=MESH
        )

    def blk(i):
        return slice(i * LANES, (i + 1) * LANES)

    c_out = [load(8 + i, out_h.at[blk(i)], out_v.at[blk(i)]) for i in range(blocks)]
    body, tail = slice(0, rows - HALO), slice(rows - HALO, rows)
    c_tail = [
        load(4, gate_h.at[tail], gate_v.at[tail]), load(5, value_h.at[tail], value_v.at[tail])
    ]
    c_gain = load(1, gain_h, gain_v)
    c_shift = load(2, shift_h, shift_v)
    c_taps = load(3, taps_h, taps_v)

    c_og = load(6, og_h, og_v)
    c_weight = [
        load(n, weight_h.at[:, cs], weight_v.at[:, cs])
        for n, cs in ((0, slice(0, NB)), (7, slice(NB, chans)))
    ]

    barrier = pltpu.get_barrier_semaphore()
    p_me = y * NX + x
    plane_dev = []
    plane_pos = []
    offsets = [(i // NX, i % NX) for i in range(1, PLANE)]
    offsets.sort(key=lambda o: -(min(o[0], NY - o[0]) + min(o[1], NX - o[1])))
    for dy, dx in offsets:
        py, px = lax.rem(y + dy, NY), lax.rem(x + dx, NX)
        plane_pos.append(py * NX + px)
        plane_dev.append({"sp_1": py, "sp_2": px})
    z_pos = [lax.rem(z + k, NZ) for k in (4, 3, 5, 2, 6, 1, 7)]
    z_dev = [{"sp_0": p} for p in z_pos]
    partners = [other, nxt, prv] + plane_dev + z_dev
    for dev in partners:
        pl.semaphore_signal(barrier, inc=1, device_id=dev, device_id_type=MESH)

    c_out[0].wait()
    c_body = [
        load(12, gate_h.at[body], gate_v.at[body]), load(13, value_h.at[body], value_v.at[body])
    ]

    def cols(g):
        return slice(g * LANES, (g + 1) * LANES)

    eye = lax.broadcasted_iota(jnp.int32, (LANES, LANES), 0) == lax.broadcasted_iota(
        jnp.int32, (LANES, LANES), 1
    )
    for i in range(blocks):
        if i:
            c_out[i].wait()
        part = out_v[blk(i), cols(0)].astype(F32)
        for g in range(1, groups):
            part = part + out_v[blk(i), cols(g)].astype(F32)
        s = jnp.sum(part, axis=1, keepdims=True)
        m = s * (1.0 / chans)
        d = out_v[blk(i), cols(0)].astype(F32) - m
        sq = d * d
        for g in range(1, groups):
            d = out_v[blk(i), cols(g)].astype(F32) - m
            sq = sq + d * d
        st_a[0, i : i + 1, :] = jnp.sum(jnp.where(eye, s, 0.0), axis=0, keepdims=True)
        st_a[0, blocks + i : blocks + i + 1, :] = jnp.sum(sq.T, axis=0, keepdims=True)

    pl.semaphore_wait(barrier, len(partners))
    c_st1 = send(st_a.at[0], st_b.at[0], st_sem.at[0], st_sem.at[1], other)

    SB = 64
    def gate_rows(lo, n):
        rs = pl.ds(lo, n)
        for g in range(groups):
            gated = value_v[rs, cols(g)].astype(F32) * sigmoid(gate_v[rs, cols(g)].astype(F32))
            gt[g, pl.ds(HALO + lo, n), :] = gated.astype(BF16).astype(F32)

    for c in c_tail:
        c.wait()
    gate_rows(rows - HALO, HALO)
    c_halo = send(
        gt.at[:, pl.ds(rows, HALO), :], gt.at[:, pl.ds(0, HALO), :],
        halo_sem.at[0], halo_sem.at[1], nxt,
    )
    c_gain.wait()
    c_shift.wait()
    c_taps.wait()
    for g in range(groups):
        tapsf[g, 0:taps_n, :] = taps_v[:, cols(g)].astype(F32)
    def act_grad(n):
        cs = pl.ds(pl.multiple_of(n * NB, NB), NB)
        sc_v[:, cs] = jnp.dot(og_v[...], weight_v[:, cs], preferred_element_type=F32)

    c_og.wait()
    c_weight[0].wait()
    act_grad(0)
    c_st1.wait_recv()

    def spread(dst, src, first=0):
        for i in range(src.shape[0]):
            dst[blk(first + i), :] = jnp.broadcast_to(src[i : i + 1, :], (LANES, LANES)).T

    own, peer = st_a[0], st_b[0]
    s0, m0 = own[0:blocks], own[blocks : 2 * blocks]
    s1, m1 = peer[0:blocks], peer[blocks : 2 * blocks]
    ds = s0 - s1
    var = (m0 + m1 + ds * ds * (1.0 / chan_total)) * (1.0 / chan_total)
    spread(cen_b, (s0 + s1) * (1.0 / chan_total))
    spread(inv_b, lax.rsqrt(var + norm_eps))

    @pl.loop(0, rows // SB)
    def _(i):
        rs = pl.ds(i * SB, SB)
        cen, inv = cen_b[rs, :], inv_b[rs, :]
        for g in range(groups):
            sh = (out_v[rs, cols(g)].astype(F32) - cen) * inv * gain_v[g : g + 1, :] + shift_v[g : g + 1, :]
            sg = sigmoid(sh)
            act = sh * sg
            act_v[rs, cols(g)] = act.astype(BF16)
            fac_v[rs, cols(g)] = sg + act * (1.0 - sg)

    zb = PLANE * 16
    third = chans // 3
    HZ = NZ // 2

    ZM = 4

    def partial(hf):
        m = ZM * zb
        lhs = og_v[:, hf * m : (hf + 1) * m]
        part = lax.dot_general(
            lhs, act_v[...], (((0,), (0,)), ((), ())), preferred_element_type=F32
        ).astype(BF16)
        for zq in range(ZM):
            for yy in range(NY):
                for xx in range(NX):
                    r0 = zq * zb + (yy * NX + xx) * 16
                    for c in range(third // LANES):
                        piece = [
                            part[r0 : r0 + 16, i * third + c * LANES : i * third + (c + 1) * LANES]
                            for i in range(3)
                        ]
                        gx[xx, hf, yy * 4 + zq, c] = piece[0]
                        gy[yy, hf, xx * 4 + zq, c] = piece[1]
                        gz[hf * ZM + zq, yy // 2, (yy % 2) * 4 + xx, c] = piece[2]

    DIRS = (1, -1)

    def tiles_add(n, step, fn):
        @pl.loop(0, n // step)
        def _(j):
            fn(j, pl.ds(j * step, step))

    class Ring4:
        def __init__(self, g, r, m, axis, pos, base, sem):
            self.g, self.r, self.m = g, r, m
            self.axis, self.pos, self.base, self.sem = axis, pos, base, sem
            self.c = {}
            self.n = r.shape[2]
            self.step = min(4, self.n)

        def go(self, h, src, slot, d):
            self.c[slot, h] = send(
                src, self.r.at[slot, h], rs_send.at[self.sem], rs_recv.at[self.base + 2 * slot + h],
                {self.axis: lax.rem(self.pos + 4 + d, 4)},
            )

        def start(self, h):
            d = DIRS[h]
            self.go(h, self.g.at[lax.rem(self.pos + 2, 4), h], 0, d)

        def single(self, h):
            d = DIRS[h]
            self.go(h, self.g.at[lax.rem(self.pos + 4 - d, 4), h], 1, -d)

        def mid(self, h):
            d = DIRS[h]
            self.c[0, h].wait_recv()
            idx = lax.rem(self.pos + 4 + d, 4)

            def fn(j, t):
                self.m[h, t] = (self.r[0, h, t].astype(F32) + self.g[idx, h, t].astype(F32)).astype(BF16)

            tiles_add(self.n, self.step, fn)
            self.go(h, self.m.at[h], 2, d)

        def end(self, h, write):
            self.c[1, h].wait_recv()
            self.c[2, h].wait_recv()

            def fn(j, t):
                v = self.r[1, h, t].astype(F32) + self.r[2, h, t].astype(F32) + self.g[self.pos, h, t].astype(F32)
                write(h, j, v.astype(BF16))

            tiles_add(self.n, self.step, fn)

        def drain(self):
            total(self.r, rs_send.at[self.sem], rs_recv.at[self.base]).wait_send()

    class Ring8:
        def __init__(self, base, sem):
            self.base, self.sem = base, sem
            self.c = {}

        def g(self, h, k):
            return gz.at[lax.rem(z + 16 + k * DIRS[h], NZ), h]

        def go(self, h, src, slot, d):
            self.c[slot, h] = send(
                src, r_z.at[slot, h], rs_send.at[self.sem], rs_recv.at[self.base + 2 * slot + h],
                {"sp_0": lax.rem(z + NZ + d, NZ)},
            )

        def start(self, h):
            d = DIRS[h]
            self.go(h, self.g(h, 4), 0, d)
            self.go(h, self.g(h, -3), 4, -d)

        def hop(self, h, slot, k, d):
            self.c[slot, h].wait_recv()
            own = self.g(h, k)
            q = slot if slot < 4 else slot - 1

            def fn(j, t):
                mz[q, h, t] = (r_z[slot, h, t].astype(F32) + own[t].astype(F32)).astype(BF16)

            tiles_add(8, 4, fn)
            self.go(h, mz.at[q, h], slot + 1, d)

        def long(self, h, r):
            self.hop(h, r - 1, 4 - r, DIRS[h])

        def short(self, h, r):
            self.hop(h, 3 + r, r - 3, -DIRS[h])

        def end(self, h):
            self.c[3, h].wait_recv()
            self.c[6, h].wait_recv()

            def fn(j, t):
                v = r_z[3, h, t].astype(F32) + r_z[6, h, t].astype(F32) + gz[z, h, t].astype(F32)
                hz[pl.ds(h * 8 + j * 4, 4)] = v.astype(BF16)

            tiles_add(8, 4, fn)

        def drain(self):
            total(r_z, rs_send.at[self.sem], rs_recv.at[self.base]).wait_send()

    rx = Ring4(gx, r_x, mx, "sp_2", x, 0, 0)
    ry = Ring4(gy, r_y, my, "sp_1", y, 6, 1)
    qx = Ring4(hx, s_x, m2x, "sp_1", y, 12, 2)
    qy = Ring4(hy, s_y, m2y, "sp_2", x, 18, 3)
    rz = Ring8(24, 4)

    for hf in range(2):
        partial(hf)
        rx.start(hf)
        ry.start(hf)
    for hf in range(2):
        rz.start(hf)
    for hf in range(2):
        rx.single(hf)
        ry.single(hf)

    c_weight[1].wait()
    pl.loop(1, chans // NB)(act_grad)

    zero = jnp.zeros((8, LANES), F32)

    def norm_pass(i, carry):
        rs = pl.ds(i * SB, SB)
        cen, inv = cen_b[rs, :], inv_b[rs, :]
        r_sum = jnp.zeros((SB, LANES), F32)
        r_dot = jnp.zeros((SB, LANES), F32)
        new = []
        for g in range(groups):
            n = sc_v[rs, cols(g)] * fac_v[rs, cols(g)]
            xc = (out_v[rs, cols(g)].astype(F32) - cen) * inv
            nx = n * xc
            new.append(carry[2 * g] + jnp.sum(nx.reshape(SB // 8, 8, LANES), axis=0))
            new.append(carry[2 * g + 1] + jnp.sum(n.reshape(SB // 8, 8, LANES), axis=0))
            sc = n * gain_v[g : g + 1, :]
            r_sum = r_sum + sc
            r_dot = r_dot + sc * xc
            sc_v[rs, cols(g)] = sc
        sum_b[rs, :] = r_sum
        dot_b[rs, :] = r_dot
        return tuple(new)

    sums = (zero,) * (2 * groups)
    hb = blocks // 2
    hi = rows // SB // 2
    c_st2 = []
    for q in range(2):
        sums = lax.fori_loop(q * hi, (q + 1) * hi, norm_pass, sums)
        for i in range(hb):
            k = q * hb + i
            st_a[1 + q, i : i + 1, :] = jnp.sum(sum_b[blk(k), :].T, axis=0, keepdims=True)
            st_a[1 + q, hb + i : hb + i + 1, :] = jnp.sum(dot_b[blk(k), :].T, axis=0, keepdims=True)
        c_st2.append(send(
            st_a.at[1 + q], st_b.at[1 + q], st_sem.at[2 + 2 * q], st_sem.at[3 + 2 * q], other
        ))

    def put_row(g, j, row):
        red[(g * AUX + j) // 8, j % 8 : j % 8 + 1, :] = row

    for g in range(groups):
        put_row(g, taps_n, jnp.sum(sums[2 * g], axis=0, keepdims=True))
        put_row(g, taps_n + 1, jnp.sum(sums[2 * g + 1], axis=0, keepdims=True))
        for j in range(taps_n + 2, AUX):
            put_row(g, j, jnp.zeros((1, LANES), F32))
    for t in range(groups * AUX // 8, red.shape[0]):
        red[t] = zero

    for c in c_body:
        c.wait()
    GB = 96
    pl.loop(0, (rows - HALO) // GB)(lambda i: gate_rows(pl.multiple_of(i * GB, GB), GB))
    for q in range(2):
        c_st2[q].wait_recv()
        both = (st_a[1 + q] + st_b[1 + q]) * (1.0 / chan_total)
        spread(sum_b, both[0:hb], q * hb)
        spread(dot_b, both[hb : 2 * hb], q * hb)

        @pl.loop(q * hi, (q + 1) * hi)
        def _(i):
            rs = pl.ds(i * SB, SB)
            cen, inv = cen_b[rs, :], inv_b[rs, :]
            gs, gd = sum_b[rs, :], dot_b[rs, :]
            for g in range(groups):
                xc = (out_v[rs, cols(g)].astype(F32) - cen) * inv
                hg[g, rs, :] = inv * (sc_v[rs, cols(g)] - gs - xc * gd)

    for g in range(groups):
        edge[g] = hg[g, 0:HALO, :].astype(BF16)
    rx.mid(0)
    ry.mid(0)
    for h in range(2):
        rz.long(h, 1)

    c_halo.wait_recv()

    @pl.when(place == 0)
    def _():
        gt[:, 0:HALO, :] = jnp.zeros((groups, HALO, LANES), F32)

    UB = 8
    UT = 16

    def taps_part(lo, hi):
        @pl.loop(lo, hi)
        def _(g):
            def step(t, acc):
                base = pl.multiple_of(t * (8 * UT), 8 * UT)
                hs = [hg[g, pl.ds(base + 8 * b, 8), :] for b in range(UT)]
                acc = list(acc)
                for o in range(taps_n + 8 * (UT - 1)):
                    v = gt[g, pl.ds(base + (HALO - reach + o), 8), :]
                    for b in range(UT):
                        if 0 <= o - 8 * b < taps_n:
                            acc[o - 8 * b] = acc[o - 8 * b] + hs[b] * v
                return tuple(acc)

            acc = lax.fori_loop(0, rows // (8 * UT), step, (zero,) * taps_n)
            for j in range(taps_n):
                red[g * (AUX // 8) + j // 8, j % 8 : j % 8 + 1, :] = jnp.sum(
                    acc[j], axis=0, keepdims=True
                )

    TB = 8 * UB

    def gated_part(lo, hi):
        @pl.loop(0, groups)
        def _(g):
            weights = [jnp.broadcast_to(tapsf[g, j : j + 1, :], (8, LANES)) for j in range(taps_n)]
            cs = pl.ds(pl.multiple_of(g * LANES, LANES), LANES)

            @pl.loop(lo, hi)
            def _(t):
                base = pl.multiple_of(t * TB, TB)
                parts = [None] * UB
                for o in range(taps_n + TB - 8):
                    v = hg[g, pl.ds(base + o, 8), :]
                    for b in range(UB):
                        j = 8 * b + reach - o
                        if 0 <= j < taps_n:
                            term = weights[j] * v
                            parts[b] = term if parts[b] is None else parts[b] + term
                gg = jnp.concatenate(parts, axis=0)
                rs = pl.ds(base, TB)
                sg = sigmoid(gate_v[rs, cs].astype(F32))
                val = value_v[rs, cs].astype(F32)
                gs = gg * sg
                gv_v[rs, cs] = gs.astype(BF16)
                gg_v[rs, cs] = (gs * val * (1.0 - sg)).astype(BF16)

    def to_hx(h, j, v):
        hx[j, h] = v

    def to_hy(h, j, v):
        hy[j, h] = v

    def to_e(e):
        def write(h, j, v):
            e[h * HZ : (h + 1) * HZ] = v

        return write

    def send_z(i, e, zr, h):
        for p in range(h * HZ, (h + 1) * HZ):

            @pl.when(z != p)
            def _(p=p):
                send(e.at[p], zr.at[z], z_send.at[i], z_recv.at[i], {"sp_0": p})

    taps_part(0, 1)
    rx.mid(1)
    ry.mid(1)
    c_back = send(edge, edge_r, halo_sem.at[2], halo_sem.at[3], prv)
    for h in range(2):
        rz.short(h, 1)
    taps_part(1, groups)
    for k in range(1, PLANE):
        send(
            red.at[pl.ds(2 * plane_pos[k - 1], 2)], red_r.at[k - 1],
            ar_send.at[0], ar_recv.at[0], plane_dev[k - 1],
        )
    for h in range(2):
        rz.long(h, 2)
    gated_part(0, 1)
    rx.end(0, to_hx)
    qx.start(0)
    qx.single(0)
    ry.end(0, to_hy)
    qy.start(0)
    qy.single(0)
    for h in range(2):
        rz.short(h, 2)
    gated_part(1, 2)
    rx.end(1, to_hx)
    qx.start(1)
    qx.single(1)
    ry.end(1, to_hy)
    qy.start(1)
    qy.single(1)
    gated_part(2, 3)
    for h in range(2):
        rz.long(h, 3)
    qx.mid(0)
    qy.mid(0)
    gated_part(3, 4)
    total(red_r, ar_send.at[0], ar_recv.at[0]).wait_recv()
    mine = red[pl.ds(2 * p_me, 2)]
    for k in range(PLANE - 1):
        mine = mine + red_r[k]
    zred[z] = mine
    for k in range(1, NZ):
        send(zred.at[z], zred.at[z], ar_send.at[1], ar_recv.at[1], z_dev[k - 1])
    gated_part(4, 5)
    qx.mid(1)
    qy.mid(1)
    gated_part(5, 7)
    c_back.wait_recv()
    for g in range(groups):
        hg[g, rows : rows + HALO, :] = jnp.where(place == last - 1, 0.0, edge_r[g].astype(F32))
    gated_part(7, 8)
    qx.end(0, to_e(ex))
    send_z(0, ex, zx, 0)
    qy.end(0, to_e(ey))
    send_z(1, ey, zy, 0)
    for h in range(2):
        rz.end(h)
    for k in range(1, PLANE):
        send(
            hz.at[plane_pos[k - 1]], pz.at[k - 1], z_send.at[2], z_recv.at[2], plane_dev[k - 1],
        )
    qx.end(1, to_e(ex))
    send_z(0, ex, zx, 1)
    qy.end(1, to_e(ey))
    send_z(1, ey, zy, 1)

    total(zred.at[0 : NZ - 1], ar_send.at[1], ar_recv.at[1]).wait_recv()
    tot = zred[0]
    for k in range(1, NZ):
        tot = tot + zred[k]
    ag[pl.ds(2 * p_me, 2)] = tot
    for k in range(1, PLANE):
        send(
            ag.at[pl.ds(2 * p_me, 2)], ag.at[pl.ds(2 * p_me, 2)],
            ar_send.at[2], ar_recv.at[2], plane_dev[k - 1],
        )

    total(pz, z_send.at[2], z_recv.at[2]).wait_recv()
    t = hz[p_me].astype(F32)
    for k in range(PLANE - 1):
        t = t + pz[k].astype(F32)
    def put_proj(i, t):
        for c in range(third // LANES):
            gproj_o[:, i * third + c * LANES : i * third + (c + 1) * LANES] = t[c]

    put_proj(2, t)

    total(ag.at[0 : 2 * PLANE - 2], ar_send.at[2], ar_recv.at[2]).wait_recv()
    for g in range(groups):
        for u in range(AUX // 8):
            tile = ag[g * (AUX // 8) + u]
            if u < taps_n // 8:
                gtaps_o[u * 8 : u * 8 + 8, cols(g)] = tile
            elif u == taps_n // 8:
                gtaps_o[u * 8 : taps_n, cols(g)] = tile[0 : taps_n - u * 8]
        for j, o in ((taps_n, ggain_o), (taps_n + 1, gshift_o)):
            o[g : g + 1, :] = ag[(g * AUX + j) // 8, j % 8 : j % 8 + 1, :]

    for i, (e, zr) in enumerate(((ex, zx), (ey, zy))):
        total(zr.at[0 : NZ - 1], z_send.at[i], z_recv.at[i]).wait_recv()
        zr[z] = e[z]
        t = zr[0].astype(F32)
        for k in range(1, NZ):
            t = t + zr[k].astype(F32)
        put_proj(i, t)

    for c in (c_st1, *c_st2, c_halo, c_back):
        c.wait_send()
    for q in (rx, ry, qx, qy, rz):
        q.drain()
    for i, ref in enumerate((red_r, zred.at[0 : NZ - 1], ag.at[0 : 2 * PLANE - 2])):
        total(ref, ar_send.at[i], ar_recv.at[i]).wait_send()
    for i, ref in enumerate((zx.at[0 : NZ - 1], zy.at[0 : NZ - 1], pz)):
        total(ref, z_send.at[i], z_recv.at[i]).wait_send()


def put_kernel(*refs):
    n = len(refs) // 2
    sem = refs[-1]
    copies = [pltpu.make_async_copy(refs[i], refs[n + i], sem.at[i]) for i in range(n)]
    for c in copies:
        c.start()
    for c in copies:
        c.wait()


def local(conv_value, conv_gate, conv_out, conv_taps, norm_gain, norm_shift, proj_weight, out_grad):
    rows, chans = conv_value.shape
    taps_n = conv_taps.shape[0]
    d_model = proj_weight.shape[0]
    groups = chans // LANES
    third = chans // 3
    hbm_s = pl.BlockSpec(memory_space=pltpu.HBM)
    vm_s = pl.BlockSpec(memory_space=pltpu.VMEM)
    V = pltpu.VMEM
    DMA = pltpu.SemaphoreType.DMA

    def color():
        return [
            V((4, 2, 16, third // LANES, 16, LANES), BF16), V((3, 2, 16, third // LANES, 16, LANES), BF16), V((2, 16, third // LANES, 16, LANES), BF16),
            V((4, 2, 4, third // LANES, 16, LANES), BF16), V((3, 2, 4, third // LANES, 16, LANES), BF16), V((2, 4, third // LANES, 16, LANES), BF16),
            V((NZ, third // LANES, 16, LANES), BF16), V((NZ, third // LANES, 16, LANES), BF16),
        ]

    scratch = [
        V((rows, chans), BF16), V((rows, chans), BF16), V((rows, chans), BF16),
        V((taps_n, chans), BF16), V((groups, LANES), F32), V((groups, LANES), F32),
        V((d_model, chans), BF16), V((rows, d_model), BF16), DMA((14,)),
        V((3, 8, LANES), F32), V((3, 8, LANES), F32),
        *[V((rows, LANES), F32)] * 4,
        V((rows, chans), BF16), V((rows, chans), F32), V((rows, chans), F32),
        V((groups, rows + HALO, LANES), F32), V((groups, rows + HALO, LANES), F32),
        V((groups, 32, LANES), F32), V((groups, HALO, LANES), BF16), V((groups, HALO, LANES), BF16),
        *color(), *color(),
        V((NZ, 2, 8, third // LANES, 16, LANES), BF16), V((7, 2, 8, third // LANES, 16, LANES), BF16), V((5, 2, 8, third // LANES, 16, LANES), BF16),
        V((PLANE, third // LANES, 16, LANES), BF16), V((PLANE - 1, third // LANES, 16, LANES), BF16),
        V((2 * PLANE, 8, LANES), F32), V((PLANE - 1, 2, 8, LANES), F32), V((NZ, 2, 8, LANES), F32),
        V((2 * PLANE, 8, LANES), F32),
        DMA((6,)), DMA((4,)), DMA((5,)), DMA((38,)), DMA((3,)), DMA((3,)), DMA((3,)), DMA((3,)),
    ]
    S = jax.ShapeDtypeStruct
    shapes = (
        S((rows, chans), BF16), S((rows, chans), BF16), S((taps_n, chans), F32),
        S((groups, LANES), F32), S((groups, LANES), F32), S((16, chans), F32),
    )
    held = pl.pallas_call(
        kernel,
        name="conv_backward",
        out_shape=shapes,
        in_specs=[hbm_s] * 8,
        out_specs=(vm_s,) * 6,
        scratch_shapes=scratch,
        compiler_params=pltpu.CompilerParams(
            collective_id=0, has_side_effects=True, vmem_limit_bytes=VMEM_LIMIT
        ),
    )(*(
        pltpu.with_memory_space_constraint(a, pltpu.HBM)
        for a in (
            conv_value, conv_gate, conv_out, conv_taps,
            norm_gain.reshape(groups, LANES), norm_shift.reshape(groups, LANES), proj_weight, out_grad,
        )
    ))
    gv, gg, gtaps, ggain, gshift, gproj = pl.pallas_call(
        put_kernel,
        name="put_outputs",
        out_shape=shapes,
        in_specs=[vm_s] * len(shapes),
        out_specs=(hbm_s,) * len(shapes),
        scratch_shapes=[DMA((len(shapes),))],
        compiler_params=pltpu.CompilerParams(vmem_limit_bytes=1024 * 1024),
    )(*held)
    return gv, gg, gtaps, ggain.reshape(chans), gshift.reshape(chans), gproj


def solution(mesh):
    split = Mesh(mesh.devices.reshape(8, 4, 4, mesh.shape["tp"]), (*SP, "tp"))
    placed = (
        P(SP, "tp"), P(SP, "tp"), P(SP, "tp"), P(None, "tp"),
        P("tp"), P("tp"), P(None, "tp"), P(SP, None),
    )
    return jax.shard_map(
        local,
        mesh=split,
        in_specs=placed,
        out_specs=(P(SP, "tp"), P(SP, "tp"), P(None, "tp"), P("tp"), P("tp"), P(SP, "tp")),
        check_vma=False,
    )
```

```python
import jax
import jax.numpy as jnp
from jax import lax
from jax.experimental import pallas as pl
from jax.experimental.pallas import tpu as pltpu
from jax.sharding import Mesh
from jax.sharding import PartitionSpec as P

SP = ("sp_0", "sp_1", "sp_2")
MESH = pl.DeviceIdType.MESH
F32, BF16 = jnp.float32, jnp.bfloat16

norm_eps = 1e-05
LANES = 128
HALO = 32
AUX = 40
NX = NY = 4
NZ = 8
PLANE = NX * NY
VMEM_LIMIT = 32 * 1024 * 1024


def sigmoid(v):
    return 0.5 + 0.5 * jnp.tanh(0.5 * v)


def kernel(
    value_h, gate_h, out_h, taps_h, gain_h, shift_h, weight_h, og_h,
    gv_v, gg_v, gtaps_o, ggain_o, gshift_o, gproj_o,
    value_v, gate_v, out_v, taps_v, gain_v, shift_v, weight_v, og_v, in_sem,
    st_a, st_b, cen_b, inv_b, sum_b, dot_b, act_v, fac_v, sc_v, hg, gt, tapsf, edge, edge_r,
    gx, r_x, mx, hx, s_x, m2x, ex, zx,
    gy, r_y, my, hy, s_y, m2y, ey, zy,
    gz, r_z, mz, hz, pz,
    red, red_r, zred, ag,
    st_sem, halo_sem, rs_send, rs_recv, z_send, z_recv, ar_send, ar_recv,
):
    rows, chans = value_v.shape
    groups = chans // LANES
    taps_n = taps_v.shape[0]
    reach = taps_n - 1
    chan_total = 2.0 * chans
    z, y, x = (lax.axis_index(a) for a in SP)
    core = lax.axis_index("tp")
    place = (z * NY + y) * NX + x
    last = NZ * PLANE
    blocks = rows // LANES
    NB = 256

    def at_place(s):
        return {"sp_0": s // PLANE, "sp_1": lax.rem(s // NX, NY), "sp_2": lax.rem(s, NX)}

    nxt = at_place(lax.rem(place + 1, last))
    prv = at_place(lax.rem(place + last - 1, last))
    other = {"tp": 1 - core}

    def load(i, src, dst):
        c = pltpu.make_async_copy(src, dst, in_sem.at[i])
        c.start()
        return c

    def send(src, dst, ss, rs, dev):
        c = pltpu.make_async_remote_copy(
            src_ref=src, dst_ref=dst, send_sem=ss, recv_sem=rs, device_id=dev, device_id_type=MESH
        )
        c.start()
        return c

    def total(ref, ss, rs):
        return pltpu.make_async_remote_copy(
            src_ref=ref, dst_ref=ref, send_sem=ss, recv_sem=rs, device_id=other, device_id_type=MESH
        )

    def blk(i):
        return slice(i * LANES, (i + 1) * LANES)

    c_out = [load(8 + i, out_h.at[blk(i)], out_v.at[blk(i)]) for i in range(blocks)]
    body, tail = slice(0, rows - HALO), slice(rows - HALO, rows)
    c_tail = [
        load(4, gate_h.at[tail], gate_v.at[tail]), load(5, value_h.at[tail], value_v.at[tail])
    ]
    c_gain = load(1, gain_h, gain_v)
    c_shift = load(2, shift_h, shift_v)
    c_taps = load(3, taps_h, taps_v)

    c_og = load(6, og_h, og_v)
    c_weight = [
        load(n, weight_h.at[:, cs], weight_v.at[:, cs])
        for n, cs in ((0, slice(0, NB)), (7, slice(NB, chans)))
    ]

    barrier = pltpu.get_barrier_semaphore()
    p_me = y * NX + x
    plane_dev = []
    plane_pos = []
    offsets = [(i // NX, i % NX) for i in range(1, PLANE)]
    offsets.sort(key=lambda o: -(min(o[0], NY - o[0]) + min(o[1], NX - o[1])))
    for dy, dx in offsets:
        py, px = lax.rem(y + dy, NY), lax.rem(x + dx, NX)
        plane_pos.append(py * NX + px)
        plane_dev.append({"sp_1": py, "sp_2": px})
    z_pos = [lax.rem(z + k, NZ) for k in (4, 3, 5, 2, 6, 1, 7)]
    z_dev = [{"sp_0": p} for p in z_pos]
    partners = [other, nxt, prv] + plane_dev + z_dev
    for dev in partners:
        pl.semaphore_signal(barrier, inc=1, device_id=dev, device_id_type=MESH)

    c_out[0].wait()
    c_body = [
        load(12, gate_h.at[body], gate_v.at[body]), load(13, value_h.at[body], value_v.at[body])
    ]

    def cols(g):
        return slice(g * LANES, (g + 1) * LANES)

    eye = lax.broadcasted_iota(jnp.int32, (LANES, LANES), 0) == lax.broadcasted_iota(
        jnp.int32, (LANES, LANES), 1
    )
    for i in range(blocks):
        if i:
            c_out[i].wait()
        part = out_v[blk(i), cols(0)].astype(F32)
        for g in range(1, groups):
            part = part + out_v[blk(i), cols(g)].astype(F32)
        s = jnp.sum(part, axis=1, keepdims=True)
        m = s * (1.0 / chans)
        d = out_v[blk(i), cols(0)].astype(F32) - m
        sq = d * d
        for g in range(1, groups):
            d = out_v[blk(i), cols(g)].astype(F32) - m
            sq = sq + d * d
        st_a[0, i : i + 1, :] = jnp.sum(jnp.where(eye, s, 0.0), axis=0, keepdims=True)
        st_a[0, blocks + i : blocks + i + 1, :] = jnp.sum(sq.T, axis=0, keepdims=True)

    pl.semaphore_wait(barrier, len(partners))
    c_st1 = send(st_a.at[0], st_b.at[0], st_sem.at[0], st_sem.at[1], other)

    SB = 128
    def gate_rows(lo, n):
        rs = pl.ds(lo, n)
        for g in range(groups):
            gated = value_v[rs, cols(g)].astype(F32) * sigmoid(gate_v[rs, cols(g)].astype(F32))
            gt[g, pl.ds(HALO + lo, n), :] = gated.astype(BF16).astype(F32)

    for c in c_tail:
        c.wait()
    gate_rows(rows - HALO, HALO)
    c_halo = send(
        gt.at[:, pl.ds(rows, HALO), :], gt.at[:, pl.ds(0, HALO), :],
        halo_sem.at[0], halo_sem.at[1], nxt,
    )
    c_gain.wait()
    c_shift.wait()
    c_taps.wait()
    for g in range(groups):
        tapsf[g, 0:taps_n, :] = taps_v[:, cols(g)].astype(F32)
    def act_grad(n):
        cs = pl.ds(pl.multiple_of(n * NB, NB), NB)
        sc_v[:, cs] = jnp.dot(og_v[...], weight_v[:, cs], preferred_element_type=F32)

    c_og.wait()
    c_weight[0].wait()
    act_grad(0)
    c_st1.wait_recv()

    def spread(dst, src, first=0):
        for i in range(src.shape[0]):
            dst[blk(first + i), :] = jnp.broadcast_to(src[i : i + 1, :], (LANES, LANES)).T

    own, peer = st_a[0], st_b[0]
    s0, m0 = own[0:blocks], own[blocks : 2 * blocks]
    s1, m1 = peer[0:blocks], peer[blocks : 2 * blocks]
    ds = s0 - s1
    var = (m0 + m1 + ds * ds * (1.0 / chan_total)) * (1.0 / chan_total)
    spread(cen_b, (s0 + s1) * (1.0 / chan_total))
    spread(inv_b, lax.rsqrt(var + norm_eps))

    @pl.loop(0, rows // SB)
    def _(i):
        rs = pl.ds(i * SB, SB)
        cen, inv = cen_b[rs, :], inv_b[rs, :]
        for g in range(groups):
            sh = (out_v[rs, cols(g)].astype(F32) - cen) * inv * gain_v[g : g + 1, :] + shift_v[g : g + 1, :]
            sg = sigmoid(sh)
            act = sh * sg
            act_v[rs, cols(g)] = act.astype(BF16)
            fac_v[rs, cols(g)] = sg + act * (1.0 - sg)

    zb = PLANE * 16
    third = chans // 3
    HZ = NZ // 2

    ZM = 4

    def partial(hf, thirds):
        m = ZM * zb
        lo = thirds[0] * third
        part = lax.dot_general(
            og_v[:, hf * m : (hf + 1) * m], act_v[:, lo : lo + len(thirds) * third],
            (((0,), (0,)), ((), ())), preferred_element_type=F32,
        ).astype(BF16)
        for zq in range(ZM):
            for yy in range(NY):
                for xx in range(NX):
                    r0 = zq * zb + (yy * NX + xx) * 16
                    for c in range(third // LANES):
                        for i in thirds:
                            c0 = i * third - lo + c * LANES
                            piece = part[r0 : r0 + 16, c0 : c0 + LANES]
                            if i == 0:
                                gx[xx, hf, yy * 4 + zq, c] = piece
                            elif i == 1:
                                gy[yy, hf, xx * 4 + zq, c] = piece
                            else:
                                gz[hf * ZM + zq, yy // 2, (yy % 2) * 4 + xx, c] = piece

    DIRS = (1, -1)

    def tiles_add(n, step, fn):
        @pl.loop(0, n // step)
        def _(j):
            fn(j, pl.ds(j * step, step))

    class Ring4:
        def __init__(self, g, r, m, axis, pos, base, sem):
            self.g, self.r, self.m = g, r, m
            self.axis, self.pos, self.base, self.sem = axis, pos, base, sem
            self.c = {}
            self.n = r.shape[2]
            self.step = min(4, self.n)

        def go(self, h, src, slot, d):
            self.c[slot, h] = send(
                src, self.r.at[slot, h], rs_send.at[self.sem], rs_recv.at[self.base + 2 * slot + h],
                {self.axis: lax.rem(self.pos + 4 + d, 4)},
            )

        def start(self, h):
            d = DIRS[h]
            self.go(h, self.g.at[lax.rem(self.pos + 2, 4), h], 0, d)

        def single(self, h):
            d = DIRS[h]
            self.go(h, self.g.at[lax.rem(self.pos + 4 - d, 4), h], 1, -d)

        def mid(self, h):
            d = DIRS[h]
            self.c[0, h].wait_recv()
            idx = lax.rem(self.pos + 4 + d, 4)

            def fn(j, t):
                self.m[h, t] = (self.r[0, h, t].astype(F32) + self.g[idx, h, t].astype(F32)).astype(BF16)

            tiles_add(self.n, self.step, fn)
            self.go(h, self.m.at[h], 2, d)

        def end(self, h, write):
            self.c[1, h].wait_recv()
            self.c[2, h].wait_recv()

            def fn(j, t):
                v = self.r[1, h, t].astype(F32) + self.r[2, h, t].astype(F32) + self.g[self.pos, h, t].astype(F32)
                write(h, j, v.astype(BF16))

            tiles_add(self.n, self.step, fn)

        def drain(self):
            total(self.r, rs_send.at[self.sem], rs_recv.at[self.base]).wait_send()

    class Ring8:
        def __init__(self, base, sem):
            self.base, self.sem = base, sem
            self.c = {}

        def g(self, h, k):
            return gz.at[lax.rem(z + 16 + k * DIRS[h], NZ), h]

        def go(self, h, src, slot, d):
            self.c[slot, h] = send(
                src, r_z.at[slot, h], rs_send.at[self.sem], rs_recv.at[self.base + 2 * slot + h],
                {"sp_0": lax.rem(z + NZ + d, NZ)},
            )

        def start(self, h):
            d = DIRS[h]
            self.go(h, self.g(h, 4), 0, d)
            self.go(h, self.g(h, -3), 4, -d)

        def hop(self, h, slot, k, d):
            self.c[slot, h].wait_recv()
            own = self.g(h, k)
            q = slot if slot < 4 else slot - 1

            def fn(j, t):
                mz[q, h, t] = (r_z[slot, h, t].astype(F32) + own[t].astype(F32)).astype(BF16)

            tiles_add(8, 4, fn)
            self.go(h, mz.at[q, h], slot + 1, d)

        def long(self, h, r):
            self.hop(h, r - 1, 4 - r, DIRS[h])

        def short(self, h, r):
            self.hop(h, 3 + r, r - 3, -DIRS[h])

        def end(self, h):
            self.c[3, h].wait_recv()
            self.c[6, h].wait_recv()

            def fn(j, t):
                v = r_z[3, h, t].astype(F32) + r_z[6, h, t].astype(F32) + gz[z, h, t].astype(F32)
                hz[pl.ds(h * 8 + j * 4, 4)] = v.astype(BF16)

            tiles_add(8, 4, fn)

        def drain(self):
            total(r_z, rs_send.at[self.sem], rs_recv.at[self.base]).wait_send()

    rx = Ring4(gx, r_x, mx, "sp_2", x, 0, 0)
    ry = Ring4(gy, r_y, my, "sp_1", y, 6, 1)
    qx = Ring4(hx, s_x, m2x, "sp_1", y, 12, 2)
    qy = Ring4(hy, s_y, m2y, "sp_2", x, 18, 3)
    rz = Ring8(24, 4)

    for hf in range(2):
        partial(hf, (0, 1))
        rx.start(hf)
        ry.start(hf)
    for hf in range(2):
        partial(hf, (2,))
    for hf in range(2):
        rz.start(hf)
    for hf in range(2):
        rx.single(hf)
        ry.single(hf)

    c_weight[1].wait()
    pl.loop(1, chans // NB)(act_grad)

    zero = jnp.zeros((8, LANES), F32)

    def norm_pass(i, carry):
        rs = pl.ds(i * SB, SB)
        cen, inv = cen_b[rs, :], inv_b[rs, :]
        r_sum = jnp.zeros((SB, LANES), F32)
        r_dot = jnp.zeros((SB, LANES), F32)
        new = []
        for g in range(groups):
            n = sc_v[rs, cols(g)] * fac_v[rs, cols(g)]
            xc = (out_v[rs, cols(g)].astype(F32) - cen) * inv
            nx = n * xc
            new.append(carry[2 * g] + jnp.sum(nx.reshape(SB // 8, 8, LANES), axis=0))
            new.append(carry[2 * g + 1] + jnp.sum(n.reshape(SB // 8, 8, LANES), axis=0))
            sc = n * gain_v[g : g + 1, :]
            r_sum = r_sum + sc
            r_dot = r_dot + sc * xc
            sc_v[rs, cols(g)] = sc
        sum_b[rs, :] = r_sum
        dot_b[rs, :] = r_dot
        return tuple(new)

    sums = (zero,) * (2 * groups)
    hb = blocks // 2
    hi = rows // SB // 2
    c_st2 = []
    for q in range(2):
        sums = lax.fori_loop(q * hi, (q + 1) * hi, norm_pass, sums)
        for i in range(hb):
            k = q * hb + i
            st_a[1 + q, i : i + 1, :] = jnp.sum(sum_b[blk(k), :].T, axis=0, keepdims=True)
            st_a[1 + q, hb + i : hb + i + 1, :] = jnp.sum(dot_b[blk(k), :].T, axis=0, keepdims=True)
        c_st2.append(send(
            st_a.at[1 + q], st_b.at[1 + q], st_sem.at[2 + 2 * q], st_sem.at[3 + 2 * q], other
        ))

    def put_row(g, j, row):
        red[(g * AUX + j) // 8, j % 8 : j % 8 + 1, :] = row

    for g in range(groups):
        put_row(g, taps_n, jnp.sum(sums[2 * g], axis=0, keepdims=True))
        put_row(g, taps_n + 1, jnp.sum(sums[2 * g + 1], axis=0, keepdims=True))
        for j in range(taps_n + 2, AUX):
            put_row(g, j, jnp.zeros((1, LANES), F32))
    for t in range(groups * AUX // 8, red.shape[0]):
        red[t] = zero

    for c in c_body:
        c.wait()
    GB = 96
    pl.loop(0, (rows - HALO) // GB)(lambda i: gate_rows(pl.multiple_of(i * GB, GB), GB))
    for q in range(2):
        if q:
            rx.mid(0)
            ry.mid(0)
        c_st2[q].wait_recv()
        both = (st_a[1 + q] + st_b[1 + q]) * (1.0 / chan_total)
        spread(sum_b, both[0:hb], q * hb)
        spread(dot_b, both[hb : 2 * hb], q * hb)

        @pl.loop(q * hi, (q + 1) * hi)
        def _(i):
            rs = pl.ds(i * SB, SB)
            cen, inv = cen_b[rs, :], inv_b[rs, :]
            gs, gd = sum_b[rs, :], dot_b[rs, :]
            for g in range(groups):
                xc = (out_v[rs, cols(g)].astype(F32) - cen) * inv
                hg[g, rs, :] = inv * (sc_v[rs, cols(g)] - gs - xc * gd)

    for g in range(groups):
        edge[g] = hg[g, 0:HALO, :].astype(BF16)
    for h in range(2):
        rz.long(h, 1)

    c_halo.wait_recv()

    @pl.when(place == 0)
    def _():
        gt[:, 0:HALO, :] = jnp.zeros((groups, HALO, LANES), F32)

    UB = 8
    UT = 16

    def taps_part(lo, hi):
        @pl.loop(lo, hi)
        def _(g):
            def step(t, acc):
                base = pl.multiple_of(t * (8 * UT), 8 * UT)
                hs = [hg[g, pl.ds(base + 8 * b, 8), :] for b in range(UT)]
                acc = list(acc)
                for o in range(taps_n + 8 * (UT - 1)):
                    v = gt[g, pl.ds(base + (HALO - reach + o), 8), :]
                    for b in range(UT):
                        if 0 <= o - 8 * b < taps_n:
                            acc[o - 8 * b] = acc[o - 8 * b] + hs[b] * v
                return tuple(acc)

            acc = lax.fori_loop(0, rows // (8 * UT), step, (zero,) * taps_n)
            for j in range(taps_n):
                red[g * (AUX // 8) + j // 8, j % 8 : j % 8 + 1, :] = jnp.sum(
                    acc[j], axis=0, keepdims=True
                )

    TB = 8 * UB

    def gated_part(lo, hi):
        @pl.loop(0, groups)
        def _(g):
            weights = [jnp.broadcast_to(tapsf[g, j : j + 1, :], (8, LANES)) for j in range(taps_n)]
            cs = pl.ds(pl.multiple_of(g * LANES, LANES), LANES)

            @pl.loop(lo, hi)
            def _(t):
                base = pl.multiple_of(t * TB, TB)
                parts = [None] * UB
                for o in range(taps_n + TB - 8):
                    v = hg[g, pl.ds(base + o, 8), :]
                    for b in range(UB):
                        j = 8 * b + reach - o
                        if 0 <= j < taps_n:
                            term = weights[j] * v
                            parts[b] = term if parts[b] is None else parts[b] + term
                gg = jnp.concatenate(parts, axis=0)
                rs = pl.ds(base, TB)
                sg = sigmoid(gate_v[rs, cs].astype(F32))
                val = value_v[rs, cs].astype(F32)
                gs = gg * sg
                gv_v[rs, cs] = gs.astype(BF16)
                gg_v[rs, cs] = (gs * val * (1.0 - sg)).astype(BF16)

    def to_hx(h, j, v):
        hx[j, h] = v

    def to_hy(h, j, v):
        hy[j, h] = v

    def to_e(e):
        def write(h, j, v):
            e[h * HZ : (h + 1) * HZ] = v

        return write

    def send_z(i, e, zr, h):
        for p in range(h * HZ, (h + 1) * HZ):

            @pl.when(z != p)
            def _(p=p):
                send(e.at[p], zr.at[z], z_send.at[i], z_recv.at[i], {"sp_0": p})

    taps_part(0, 1)
    rx.mid(1)
    ry.mid(1)
    c_back = send(edge, edge_r, halo_sem.at[2], halo_sem.at[3], prv)
    for h in range(2):
        rz.short(h, 1)
    taps_part(1, groups)
    for k in range(1, PLANE):
        send(
            red.at[pl.ds(2 * plane_pos[k - 1], 2)], red_r.at[k - 1],
            ar_send.at[0], ar_recv.at[0], plane_dev[k - 1],
        )
    for h in range(2):
        rz.long(h, 2)
    gated_part(0, 1)
    rx.end(0, to_hx)
    qx.start(0)
    qx.single(0)
    ry.end(0, to_hy)
    qy.start(0)
    qy.single(0)
    for h in range(2):
        rz.short(h, 2)
    gated_part(1, 2)
    rx.end(1, to_hx)
    qx.start(1)
    qx.single(1)
    ry.end(1, to_hy)
    qy.start(1)
    qy.single(1)
    gated_part(2, 3)
    for h in range(2):
        rz.long(h, 3)
    qx.mid(0)
    qy.mid(0)
    gated_part(3, 4)
    total(red_r, ar_send.at[0], ar_recv.at[0]).wait_recv()
    mine = red[pl.ds(2 * p_me, 2)]
    for k in range(PLANE - 1):
        mine = mine + red_r[k]
    zred[z] = mine
    for k in range(1, NZ):
        send(zred.at[z], zred.at[z], ar_send.at[1], ar_recv.at[1], z_dev[k - 1])
    gated_part(4, 5)
    qx.mid(1)
    qy.mid(1)
    gated_part(5, 7)
    c_back.wait_recv()
    for g in range(groups):
        hg[g, rows : rows + HALO, :] = jnp.where(place == last - 1, 0.0, edge_r[g].astype(F32))
    gated_part(7, 8)
    qx.end(0, to_e(ex))
    send_z(0, ex, zx, 0)
    qy.end(0, to_e(ey))
    send_z(1, ey, zy, 0)
    for h in range(2):
        rz.end(h)
    for k in range(1, PLANE):
        send(
            hz.at[plane_pos[k - 1]], pz.at[k - 1], z_send.at[2], z_recv.at[2], plane_dev[k - 1],
        )
    qx.end(1, to_e(ex))
    send_z(0, ex, zx, 1)
    qy.end(1, to_e(ey))
    send_z(1, ey, zy, 1)

    total(zred.at[0 : NZ - 1], ar_send.at[1], ar_recv.at[1]).wait_recv()
    tot = zred[0]
    for k in range(1, NZ):
        tot = tot + zred[k]
    ag[pl.ds(2 * p_me, 2)] = tot
    for k in range(1, PLANE):
        send(
            ag.at[pl.ds(2 * p_me, 2)], ag.at[pl.ds(2 * p_me, 2)],
            ar_send.at[2], ar_recv.at[2], plane_dev[k - 1],
        )

    total(pz, z_send.at[2], z_recv.at[2]).wait_recv()
    t = hz[p_me].astype(F32)
    for k in range(PLANE - 1):
        t = t + pz[k].astype(F32)
    def put_proj(i, t):
        for c in range(third // LANES):
            gproj_o[:, i * third + c * LANES : i * third + (c + 1) * LANES] = t[c]

    put_proj(2, t)

    total(ag.at[0 : 2 * PLANE - 2], ar_send.at[2], ar_recv.at[2]).wait_recv()
    for g in range(groups):
        for u in range(AUX // 8):
            tile = ag[g * (AUX // 8) + u]
            if u < taps_n // 8:
                gtaps_o[u * 8 : u * 8 + 8, cols(g)] = tile
            elif u == taps_n // 8:
                gtaps_o[u * 8 : taps_n, cols(g)] = tile[0 : taps_n - u * 8]
        for j, o in ((taps_n, ggain_o), (taps_n + 1, gshift_o)):
            o[g : g + 1, :] = ag[(g * AUX + j) // 8, j % 8 : j % 8 + 1, :]

    for i, (e, zr) in enumerate(((ex, zx), (ey, zy))):
        total(zr.at[0 : NZ - 1], z_send.at[i], z_recv.at[i]).wait_recv()
        zr[z] = e[z]
        t = zr[0].astype(F32)
        for k in range(1, NZ):
            t = t + zr[k].astype(F32)
        put_proj(i, t)

    for c in (c_st1, *c_st2, c_halo, c_back):
        c.wait_send()
    for q in (rx, ry, qx, qy, rz):
        q.drain()
    for i, ref in enumerate((red_r, zred.at[0 : NZ - 1], ag.at[0 : 2 * PLANE - 2])):
        total(ref, ar_send.at[i], ar_recv.at[i]).wait_send()
    for i, ref in enumerate((zx.at[0 : NZ - 1], zy.at[0 : NZ - 1], pz)):
        total(ref, z_send.at[i], z_recv.at[i]).wait_send()


def put_kernel(*refs):
    n = len(refs) // 2
    sem = refs[-1]
    copies = [pltpu.make_async_copy(refs[i], refs[n + i], sem.at[i]) for i in range(n)]
    for c in copies:
        c.start()
    for c in copies:
        c.wait()


def local(conv_value, conv_gate, conv_out, conv_taps, norm_gain, norm_shift, proj_weight, out_grad):
    rows, chans = conv_value.shape
    taps_n = conv_taps.shape[0]
    d_model = proj_weight.shape[0]
    groups = chans // LANES
    third = chans // 3
    hbm_s = pl.BlockSpec(memory_space=pltpu.HBM)
    vm_s = pl.BlockSpec(memory_space=pltpu.VMEM)
    V = pltpu.VMEM
    DMA = pltpu.SemaphoreType.DMA

    def color():
        return [
            V((4, 2, 16, third // LANES, 16, LANES), BF16), V((3, 2, 16, third // LANES, 16, LANES), BF16), V((2, 16, third // LANES, 16, LANES), BF16),
            V((4, 2, 4, third // LANES, 16, LANES), BF16), V((3, 2, 4, third // LANES, 16, LANES), BF16), V((2, 4, third // LANES, 16, LANES), BF16),
            V((NZ, third // LANES, 16, LANES), BF16), V((NZ, third // LANES, 16, LANES), BF16),
        ]

    scratch = [
        V((rows, chans), BF16), V((rows, chans), BF16), V((rows, chans), BF16),
        V((taps_n, chans), BF16), V((groups, LANES), F32), V((groups, LANES), F32),
        V((d_model, chans), BF16), V((rows, d_model), BF16), DMA((14,)),
        V((3, 8, LANES), F32), V((3, 8, LANES), F32),
        *[V((rows, LANES), F32)] * 4,
        V((rows, chans), BF16), V((rows, chans), F32), V((rows, chans), F32),
        V((groups, rows + HALO, LANES), F32), V((groups, rows + HALO, LANES), F32),
        V((groups, 32, LANES), F32), V((groups, HALO, LANES), BF16), V((groups, HALO, LANES), BF16),
        *color(), *color(),
        V((NZ, 2, 8, third // LANES, 16, LANES), BF16), V((7, 2, 8, third // LANES, 16, LANES), BF16), V((5, 2, 8, third // LANES, 16, LANES), BF16),
        V((PLANE, third // LANES, 16, LANES), BF16), V((PLANE - 1, third // LANES, 16, LANES), BF16),
        V((2 * PLANE, 8, LANES), F32), V((PLANE - 1, 2, 8, LANES), F32), V((NZ, 2, 8, LANES), F32),
        V((2 * PLANE, 8, LANES), F32),
        DMA((6,)), DMA((4,)), DMA((5,)), DMA((38,)), DMA((3,)), DMA((3,)), DMA((3,)), DMA((3,)),
    ]
    S = jax.ShapeDtypeStruct
    shapes = (
        S((rows, chans), BF16), S((rows, chans), BF16), S((taps_n, chans), F32),
        S((groups, LANES), F32), S((groups, LANES), F32), S((16, chans), F32),
    )
    held = pl.pallas_call(
        kernel,
        name="conv_backward",
        out_shape=shapes,
        in_specs=[hbm_s] * 8,
        out_specs=(vm_s,) * 6,
        scratch_shapes=scratch,
        compiler_params=pltpu.CompilerParams(
            collective_id=0, has_side_effects=True, vmem_limit_bytes=VMEM_LIMIT
        ),
    )(*(
        pltpu.with_memory_space_constraint(a, pltpu.HBM)
        for a in (
            conv_value, conv_gate, conv_out, conv_taps,
            norm_gain.reshape(groups, LANES), norm_shift.reshape(groups, LANES), proj_weight, out_grad,
        )
    ))
    gv, gg, gtaps, ggain, gshift, gproj = pl.pallas_call(
        put_kernel,
        name="put_outputs",
        out_shape=shapes,
        in_specs=[vm_s] * len(shapes),
        out_specs=(hbm_s,) * len(shapes),
        scratch_shapes=[DMA((len(shapes),))],
        compiler_params=pltpu.CompilerParams(vmem_limit_bytes=1024 * 1024),
    )(*held)
    return gv, gg, gtaps, ggain.reshape(chans), gshift.reshape(chans), gproj


def solution(mesh):
    split = Mesh(mesh.devices.reshape(8, 4, 4, mesh.shape["tp"]), (*SP, "tp"))
    placed = (
        P(SP, "tp"), P(SP, "tp"), P(SP, "tp"), P(None, "tp"),
        P("tp"), P("tp"), P(None, "tp"), P(SP, None),
    )
    return jax.shard_map(
        local,
        mesh=split,
        in_specs=placed,
        out_specs=(P(SP, "tp"), P(SP, "tp"), P(None, "tp"), P("tp"), P("tp"), P(SP, "tp")),
        check_vma=False,
    )
```
